256 devices in a mesh: sp: 64 (over z, x, core), tp: 4 (over y).
Axes of the slice: x: 4, y: 4, z: 8, core: 2. Of those that a mesh axis runs over, the one named last changes fastest.
Arguments:
- stream: bfloat16 [16384, 2048], P('sp'), may hold values from -6 to 6
- query: bfloat16 [16384, 1024], P('sp', 'tp'), may hold values from -6 to 6
- forget_gate_logits: bfloat16 [16384, 1024], P('sp', 'tp'), may hold values from -4 to 4
- value_input_rows: bfloat16 [16384, 1024], P('sp', 'tp'), may hold values from -6 to 6
- output_gate_logits: bfloat16 [16384, 1024], P('sp', 'tp'), may hold values from -6 to 6
- forget_floor_margin: float32 [8, 128], P('tp'), as said below
- additional_fading_speed: float32 [16384, 8], P('sp', 'tp'), may hold values from -0.7 to 0, as said below
- head_norm_gain: float32 [128], replicated, may hold values from 0.1 to 1.9
- output_head_weight: bfloat16 [1024, 2048], replicated, may hold values from -0.1875 to 0.1875
- feedforward_norm_gain: float32 [2048], replicated, may hold values from 0.1 to 1.9
- selected_expert_index: int32 [16384, 2], P('sp'), may hold values from 0 to 63, all different within a row; in each aligned block of 64 rows (0 to 63, 64 to 127, ...) at most 4 rows name the same one
- selected_expert_weight: float32 [16384, 2], P(('sp', 'tp')), may hold values from 0.2 to 1
- expert_gate_weight: bfloat16 [64, 2048, 1024], P('sp', None, 'tp'), may hold values from -0.125 to 0.125
- expert_up_weight: bfloat16 [64, 2048, 1024], P('sp', None, 'tp'), may hold values from -0.125 to 0.125
- expert_down_weight: bfloat16 [64, 1024, 2048], P('sp', 'tp'), may hold values from -0.1875 to 0.1875
Outputs:
- layer_out: bfloat16 [16384, 2048], P(('sp', 'tp'))
The draws below stay inside these ranges and needn't reach their ends.
Inputs may be any that keep to these rules, and one draw needn't show every extreme that they name: `forget_floor_margin`: positive. `additional_fading_speed`: zero at most positions. `selected_expert_index`: the 2 experts of a position differ; in each aligned block of 64 positions no expert is named more than 4 times, and in every draw some expert is named exactly 4 times in some block.
All inputs are finite; a program needn't handle non-finite values.
Results may differ from the reference program's by a relative error of at most 0.006.
Values may be sent and summed in bfloat16 or wider, within the bound.
A program may use at most 64 MiB of HBM per device.

```python
import math
import jax
import jax.numpy as jnp
import numpy as np
from jax import lax

D = 2048
SCAN_LANES = 8
HEAD_DIM = 128
FF = 1024
TOPK = 2
BLOCK = 64
TOK_DEV = 256
TOKENS = 16384
EXPERTS = 64
GROUP_ROWS = 64
CAP = 4


def draw_forget_gate_logits(key, part):
    base_key, offset_key = jax.random.split(jax.random.fold_in(key, 101))
    width = SCAN_LANES * HEAD_DIM
    base = jnp.clip(jax.random.normal(base_key, (TOKENS, width), jnp.float32), -3.0, 3.0)
    offset = jax.random.uniform(offset_key, (TOKENS // TOK_DEV, 1, SCAN_LANES, 1), jnp.float32, -1.0, 1.0)
    full = base.reshape(TOKENS // TOK_DEV, TOK_DEV, SCAN_LANES, HEAD_DIM) + offset
    return full.reshape(TOKENS, width).astype(jnp.bfloat16)


def draw_forget_floor_margin(key, part):
    order_key, fast_key, slow_key = jax.random.split(jax.random.fold_in(key, 202), 3)
    slow_count = SCAN_LANES // 2
    ranking = jax.random.permutation(order_key, SCAN_LANES)
    slow = (ranking < slow_count)[:, None]
    fast_gap = jax.random.uniform(fast_key, (SCAN_LANES, HEAD_DIM), jnp.float32, 0.04, 0.12)
    slow_gap = jax.random.uniform(slow_key, (SCAN_LANES, HEAD_DIM), jnp.float32, 0.3, 1.0) / TOKENS
    return jnp.where(slow, slow_gap, fast_gap)


def draw_additional_fading_speed(key, part):
    place_key, shift_key, depth_key = jax.random.split(jax.random.fold_in(key, 303), 3)
    first = jax.random.randint(place_key, (1, 1, SCAN_LANES), 0, TOKENS)
    shift = jax.random.randint(shift_key, (1, 1, SCAN_LANES), 1, TOKENS)
    second = (first + shift) % TOKENS
    places = jnp.concatenate([first, second], axis=0)
    depths = jax.random.uniform(depth_key, (2, 1, SCAN_LANES), jnp.float32, math.log(0.5), math.log(0.8))
    positions = jnp.arange(TOKENS, dtype=jnp.int32)[None, :, None]
    return jnp.sum(jnp.where(positions == places, depths, 0.0), axis=0)


def shard_levels(own_key, shape, cuts, smallest, high):
    loudness, own = 1.0, jax.random.fold_in(own_key, 6)
    for position, shards_of in cuts:
        heights = jnp.exp(jax.random.uniform(jax.random.fold_in(own, position), (shards_of,), jnp.float32, smallest / len(cuts), high / len(cuts)))
        loudness = loudness * jnp.repeat(heights, shape[position] // shards_of).reshape([-1 if axis == position else 1 for axis in range(len(shape))])
    return loudness


def assign_block(own_key, own, number, rows, amount, top, reach, lean):
    order = jax.random.permutation(own_key, amount)
    heavy_load, ordinary = load_shares(amount, rows * top, reach, lean, True), load_shares(amount, rows * top, reach, lean, False)
    places = jnp.arange(amount)

    def named(tallies, offset_by):
        used = int((tallies > 0).sum())
        fixed = max(1, used // 4)
        moved = fixed + (places - fixed + offset_by * (used - fixed)) % max(1, amount - fixed)
        return jnp.zeros((amount,), jnp.int32).at[order[jnp.where(places < fixed, places, moved)]].set(jnp.asarray(tallies, jnp.int32))

    tallies = jnp.where(number % 4 == 0, named(heavy_load, number // 4), named(ordinary, number - number // 4 - 1))
    mixed = jax.random.permutation(jax.random.fold_in(own, 3), amount)
    donor, taker = mixed[0:amount // 2 * 2:2], mixed[1:amount // 2 * 2:2]
    room = jnp.minimum(tallies[donor] - 1, reach - tallies[taker]) // 2
    room = jnp.where((donor == order[0]) | (taker == order[0]) | (tallies[taker] == 0), 0, jnp.maximum(room, 0))
    moved = jax.random.randint(jax.random.fold_in(own, 4), (amount // 2,), 0, 1 << 20) % (room + 1)
    tallies = tallies.at[donor].add(-moved).at[taker].add(moved)
    members = jnp.searchsorted(jnp.cumsum(tallies), jnp.arange(rows * top), side="right").astype(jnp.int32)
    grid = members.reshape(top, rows).T
    grid = grid[jax.random.permutation(jax.random.fold_in(own, 1), rows)]
    offset_by = jax.random.randint(jax.random.fold_in(own, 2), (rows, 1), 0, top)
    return jnp.take_along_axis(grid, (jnp.arange(top)[None, :] + offset_by) % top, axis=1)


def load_shares(number_of, total, bound, skew, full):
    loads = [(1 << 20) // math.isqrt(standing ** skew) + 1 for standing in range(1, number_of + 1)]
    largest = bound if full else min(bound, max(-(-total // number_of), total * loads[0] // sum(loads)))
    least = 1 if total - largest >= number_of - 1 else 0
    given, rest = [largest] + [least] * (number_of - 1), total - largest - least * (number_of - 1)
    while rest > 0:
        free = [i for i in range(1, number_of) if given[i] < largest] or [i for i in range(1, number_of) if given[i] < bound]
        pool, left = sum([loads[i] for i in free]), rest
        for i in free:
            extra = min(bound - given[i], max(1, left * loads[i] // pool), rest)
            given[i] = given[i] + extra
            rest = rest - extra
    return np.array(given)


def normal_values(own_key, extent, deviation, limit, shards=(), kind=jnp.bfloat16):
    values = deviation * jax.random.normal(own_key, extent, jnp.float32)
    if shards:
        values = values * shard_levels(own_key, extent, shards, -0.22, 0.18)
    return jnp.clip(values, -limit, limit).astype(kind)


def setup_inputs(seed: int = 0) -> dict:
    streams_of = jax.random.split(jax.random.key(seed), 16)
    stream = normal_values(streams_of[0], (TOKENS, D), 1.0, 6.0, ((0, 64),))
    query = normal_values(streams_of[1], (TOKENS, SCAN_LANES * HEAD_DIM), 1.0, 6.0, ((0, 64), (1, 4)))
    forget_gate_logits = draw_forget_gate_logits(jax.random.fold_in(streams_of[15], 71), 0)
    value_input_rows = normal_values(streams_of[3], (TOKENS, SCAN_LANES * HEAD_DIM), 1.0, 6.0, ((0, 64), (1, 4)))
    output_gate_logits = normal_values(streams_of[4], (TOKENS, SCAN_LANES * HEAD_DIM), 1.0, 6.0, ((0, 64), (1, 4)))
    forget_floor_margin = draw_forget_floor_margin(jax.random.fold_in(streams_of[15], 71), 0)
    additional_fading_speed = draw_additional_fading_speed(jax.random.fold_in(streams_of[15], 71), 0)
    head_norm_gain = jnp.clip(1.0 + 0.18 * jax.random.normal(streams_of[7], (HEAD_DIM,), jnp.float32), 0.1, 1.9)
    output_head_weight = normal_values(streams_of[8], (SCAN_LANES * HEAD_DIM, D), (SCAN_LANES * HEAD_DIM) ** -0.5, 0.1875)
    feedforward_norm_gain = jnp.clip(1.0 + 0.18 * jax.random.normal(streams_of[9], (D,), jnp.float32), 0.1, 1.9)
    selected_expert_index_keys = jax.random.split(jax.random.fold_in(streams_of[10], 1), TOKENS // GROUP_ROWS)
    selected_expert_index_turns = jax.random.permutation(jax.random.fold_in(streams_of[10], 3), TOKENS // GROUP_ROWS)
    selected_expert_index = jax.vmap(lambda own, number: assign_block(jax.random.fold_in(streams_of[10], 2), own, number, GROUP_ROWS, EXPERTS, TOPK, CAP, 1))(selected_expert_index_keys, selected_expert_index_turns).reshape((TOKENS, TOPK))
    selected_expert_weight = jnp.clip(0.2 + 0.8 * jax.random.uniform(streams_of[11], (TOKENS, TOPK), jnp.float32) ** shard_levels(streams_of[11], (TOKENS, TOPK), ((0, 256),), -0.2, 0.2), 0.2, 1.0)
    expert_gate_weight = normal_values(streams_of[12], (EXPERTS, D, FF), D ** -0.5, 0.125, ((0, 64), (2, 4)))
    expert_up_weight = normal_values(streams_of[13], (EXPERTS, D, FF), D ** -0.5, 0.125, ((0, 64), (2, 4)))
    expert_down_weight = normal_values(streams_of[14], (EXPERTS, FF, D), FF ** -0.5, 0.1875, ((0, 64), (1, 4)))
    return {"stream": stream, "query": query, "forget_gate_logits": forget_gate_logits, "value_input_rows": value_input_rows, "output_gate_logits": output_gate_logits, "forget_floor_margin": forget_floor_margin, "additional_fading_speed": additional_fading_speed, "head_norm_gain": head_norm_gain, "output_head_weight": output_head_weight, "feedforward_norm_gain": feedforward_norm_gain, "selected_expert_index": selected_expert_index, "selected_expert_weight": selected_expert_weight, "expert_gate_weight": expert_gate_weight, "expert_up_weight": expert_up_weight, "expert_down_weight": expert_down_weight}


EPS = 1e-06
HIGH = lax.Precision.HIGHEST

def cut_to_segments(array, heads):
    width = array.shape[1] // heads
    shaped = array.astype(jnp.float32).reshape(TOKENS // BLOCK, BLOCK, heads, width)
    return jnp.transpose(shaped, (0, 2, 1, 3))

def reference(stream, query, forget_gate_logits, value_input_rows, output_gate_logits, forget_floor_margin, additional_fading_speed, head_norm_gain, output_head_weight, feedforward_norm_gain, selected_expert_index, selected_expert_weight, expert_gate_weight, expert_up_weight, expert_down_weight):
    f32 = jnp.float32
    query_blk = cut_to_segments(query, SCAN_LANES)
    scores_segment_slice = cut_to_segments(forget_gate_logits, SCAN_LANES)
    value_blk = cut_to_segments(value_input_rows, SCAN_LANES)
    spike_segment_slice = cut_to_segments(additional_fading_speed, SCAN_LANES)
    clearance_amount = forget_floor_margin[None, :, None, :]
    logarithmic_fading_speed = jnp.logaddexp(jnp.log1p(-clearance_amount), jnp.log(clearance_amount) + jax.nn.log_sigmoid(scores_segment_slice)) + spike_segment_slice
    key_in = clearance_amount * jax.nn.sigmoid(-scores_segment_slice)
    causal = jnp.tril(jnp.ones((BLOCK, BLOCK), dtype=bool))[:, :, None]

    def step(state, pieces):
        query_b, key_b, value_b, log_b = pieces
        cumul = jnp.cumsum(log_b, axis=1)
        pair_log = cumul[:, :, None, :] - cumul[:, None, :, :]
        decay = jnp.exp(jnp.where(causal, pair_log, -jnp.inf))
        scores = lax.optimization_barrier(jnp.sum(query_b[:, :, None, :] * key_b[:, None, :, :] * decay, axis=-1))
        result = jnp.einsum('hts,hse->hte', scores, value_b, precision=HIGH)
        result = result + jnp.einsum('htd,hde->hte', query_b * jnp.exp(cumul), state, precision=HIGH)
        last = cumul[:, -1:, :]
        state = jnp.exp(last)[:, 0, :, None] * state + jnp.einsum('hsd,hse->hde', key_b * jnp.exp(last - cumul), value_b, precision=HIGH)
        return (state, result)
    start_state = jnp.zeros((SCAN_LANES, HEAD_DIM, HEAD_DIM), f32)
    _, recur = lax.scan(step, start_state, (query_blk, key_in, value_blk, logarithmic_fading_speed))
    recur = jnp.transpose(recur, (0, 2, 1, 3)).reshape(TOKENS, SCAN_LANES, HEAD_DIM)
    scale = lax.rsqrt(lax.optimization_barrier(jnp.mean(recur * recur, axis=-1, keepdims=True)) + EPS)
    gate_in = output_gate_logits.astype(f32).reshape(TOKENS, SCAN_LANES, HEAD_DIM)
    gated = (recur * scale * head_norm_gain * jax.nn.silu(gate_in)).astype(jnp.bfloat16).reshape(TOKENS, SCAN_LANES * HEAD_DIM)
    projected = jnp.dot(gated, output_head_weight, preferred_element_type=f32)
    mixed = (stream.astype(f32) + projected).astype(jnp.bfloat16)
    mixed_wide = lax.optimization_barrier(mixed).astype(f32)
    normed = (mixed_wide * lax.rsqrt(lax.optimization_barrier(jnp.mean(mixed_wide * mixed_wide, axis=-1, keepdims=True)) + EPS) * feedforward_norm_gain).astype(jnp.bfloat16)
    block_rows = 128
    assigned = TOKENS * TOPK
    flat_expert = selected_expert_index.reshape(-1)
    order = jnp.argsort(flat_expert, stable=True)
    sorted_expert = flat_expert[order]
    owner = order // TOPK
    counts = jnp.bincount(flat_expert, length=EXPERTS)
    padded_counts = (counts + block_rows - 1) // block_rows * block_rows
    padded_end = jnp.cumsum(padded_counts)
    padded_start = padded_end - padded_counts
    first = jnp.cumsum(counts) - counts
    dest = padded_start[sorted_expert] + jnp.arange(assigned, dtype=jnp.int32) - first[sorted_expert]
    block_count = -(-assigned // block_rows) + EXPERTS
    buffer = jnp.zeros((block_count * block_rows, D), jnp.bfloat16).at[dest].set(normed[owner])
    block_expert = jnp.minimum(jnp.searchsorted(padded_end, jnp.arange(block_count) * block_rows, side='right'), EXPERTS - 1).astype(jnp.int32)

    def expert_block(pieces):
        rows, expert = pieces
        gate_part = jnp.dot(rows, expert_gate_weight[expert], preferred_element_type=f32)
        up_part = jnp.dot(rows, expert_up_weight[expert], preferred_element_type=f32)
        hidden = (jax.nn.silu(gate_part) * up_part).astype(jnp.bfloat16)
        return jnp.dot(hidden, expert_down_weight[expert], preferred_element_type=f32).astype(jnp.bfloat16)
    outputs = lax.map(expert_block, (buffer.reshape(block_count, block_rows, D), block_expert)).reshape(-1, D)
    weighted = outputs[dest].astype(f32) * selected_expert_weight.reshape(-1)[order][:, None]
    routed = jax.ops.segment_sum(weighted, owner, num_segments=TOKENS)
    return (mixed_wide + routed).astype(jnp.bfloat16)
```

```python
import functools

import jax
import jax.numpy as jnp
from jax import lax
from jax.experimental import pallas as pl
from jax.experimental.pallas import tpu as pltpu
from jax.sharding import Mesh
from jax.sharding import PartitionSpec as P

SP = ("sp_0", "sp_1", "sp_2")
SP_TP = ("sp_0", "sp_1", "sp_2", "tp")
EPS = 1e-06
f32 = jnp.float32
bf16 = jnp.bfloat16
NZ, NX, NC, NY = 8, 4, 2, 4
ROWS = 256
GROUP = 64
CAP = 4
NT = (((1,), (1,)), ((), ()))


def dot(a, b):
    return jnp.dot(a, b, preferred_element_type=f32)


def dot_nt(a, b):
    return lax.dot_general(a, b, NT, preferred_element_type=f32)


def split2(x):
    high = x.astype(bf16)
    return high, (x - high.astype(f32)).astype(bf16)


def split3(x):
    high = x.astype(bf16)
    rest = x - high.astype(f32)
    mid = rest.astype(bf16)
    return high, mid, (rest - mid.astype(f32)).astype(bf16)


def product_nt(a, b):
    ah, al = split2(a)
    bh, bl = split2(b)
    return dot_nt(jnp.concatenate([ah, ah, al], axis=1), jnp.concatenate([bh, bl, bh], axis=1))


def ring_step(n):
    return (NZ + ((n + 1) // 2) * (1 - 2 * ((n + 1) % 2))) % NZ


def remote(src, dst, send_sem, recv_sem, device):
    return pltpu.make_async_remote_copy(
        src_ref=src,
        dst_ref=dst,
        send_sem=send_sem,
        recv_sem=recv_sem,
        device_id=device,
        device_id_type=pl.DeviceIdType.MESH,
    )


def take(ref, sem):
    pltpu.make_async_copy(ref, ref, sem).wait()


def kernel(
    dest_ref, base_ref, wsel_ref, mar_ref, fade_ref, hg_ref, fg_ref,
    q_hbm, f_hbm, v_hbm, og_hbm, stream_hbm, wh_hbm, wg_hbm, wu_hbm, wd_hbm,
    out_ref,
    qb, fb, vb, ob, stream, wh, wg, wu, wd,
    rec, qend, st_send, st_recv, tq, xr, px, us, zr, isend, inc,
    gall, acc, mixed, normed, sbuf, xbuf, hsend, hrec, rsend, rbuf, picks,
    load_sem, s_sem, c_sem, gm, gp, gr, wm, wp, wr, xs, yfm, yfp, yrm, yrp, hs, rs,
):
    z, x, c, p = [lax.axis_index(name) for name in SP_TP]
    up, down, far = (p + 1) % NY, (p + NY - 1) % NY, (p + 2) % NY
    at_up, at_down = {"tp": up}, {"tp": down}

    loads = [
        pltpu.make_async_copy(src, dst, load_sem.at[k])
        for k, (src, dst) in enumerate(
            [
                (f_hbm, fb), (q_hbm, qb), (v_hbm, vb), (wd_hbm, wd.at[p]), (og_hbm, ob),
                (wh_hbm, wh), (stream_hbm, stream), (wg_hbm, wg), (wu_hbm, wu),
            ]
        )
    ]
    for load in loads:
        load.start()

    barrier = pltpu.get_barrier_semaphore()

    def greet(k, _):
        dz, dx, dc = k // 8, (k // 2) % 4, k % 2
        pl.semaphore_signal(
            barrier,
            inc=1,
            device_id={"sp_0": (z + dz) % NZ, "sp_1": (x + dx) % NX, "sp_2": (c + dc) % NC},
            device_id_type=pl.DeviceIdType.MESH,
        )
        return 0

    lax.fori_loop(1, NZ * NX * NC, greet, 0)
    for peer in (up, down, far):
        pl.semaphore_signal(
            barrier, inc=1, device_id={"tp": peer}, device_id_type=pl.DeviceIdType.MESH
        )

    row = lax.broadcasted_iota(jnp.int32, (ROWS, ROWS), 0)
    col = lax.broadcasted_iota(jnp.int32, (ROWS, ROWS), 1)

    def ones_where(condition):
        return jnp.where(condition, 1.0, 0.0).astype(bf16)

    def level_sum(shift):
        odd = ((row >> shift) & 1) == 1
        same = (row >> shift) == (col >> shift)
        return ones_where(same & ((odd & (col <= row)) | (jnp.logical_not(odd) & (col > row))))

    loads[0].wait()
    margin = mar_ref[...]
    keys = margin * jax.nn.sigmoid(-fb[...].astype(f32))
    fade = fade_ref[...]
    fades = jnp.concatenate(
        [jnp.broadcast_to(fade[:, h : h + 1], (ROWS, 128)) for h in range(2)], axis=1
    )
    log_decay = jnp.log1p(-keys) + fades
    parts = jnp.concatenate(split3(log_decay), axis=1)

    def sums(matrix):
        three = dot(matrix, parts)
        return three[:, 0:256] + (three[:, 256:512] + three[:, 512:768])

    loads[1].wait()
    loads[2].wait()
    queries = qb[...].astype(f32)
    to_start = sums(ones_where(col <= row))
    to_end = sums(ones_where(col > row))
    qend[...] = queries * jnp.exp(to_start)
    kend = keys * jnp.exp(to_end)
    total = jnp.exp(to_start[ROWS - 1 : ROWS, :])
    vt = jnp.transpose(vb[...].astype(f32), (1, 0)).astype(bf16)
    for h in range(2):
        lanes = slice(128 * h, 128 * (h + 1))
        kh, kl = split2(kend[:, lanes])
        both = dot(vt[lanes, :], jnp.concatenate([kh, kl], axis=1))
        st_send[h, 0:128, :] = both[:, 0:128] + both[:, 128:256]
        st_send[h, 128:136, :] = jnp.broadcast_to(total[:, lanes], (8, 128))

    pl.semaphore_wait(barrier, NZ * NX * NC - 1 + 3)

    to_core = remote(st_send, st_recv, s_sem.at[0], c_sem.at[0], {"sp_2": 1 - c})
    to_core.start()
    loads[3].wait()
    for half in range(2):
        rows = pl.ds(128 * half, 128)
        other = pl.ds(128 * (1 - half), 128)
        remote(wd.at[p, rows], wd.at[p, rows], s_sem.at[1], wm.at[half], at_up).start()
        remote(wd.at[p, other], wd.at[p, other], s_sem.at[1], wp.at[1 - half], at_down).start()

    def inside(h):
        lanes = slice(128 * h, 128 * (h + 1))
        qh, kh = queries[:, lanes], keys[:, lanes]
        exponent = sums_of[3][:, lanes]
        odd = ((row[:, 0:128] >> 3) & 1) == 1
        exponent = jnp.where(odd, exponent, -exponent)
        scores = product_nt(qh * jnp.exp(exponent), kh * jnp.exp(-exponent))
        scores = jnp.where(((row >> 4) == (col >> 4)) & (col <= row), scores, 0.0)
        for shift in (4, 5, 6, 7):
            weight = jnp.exp(sums_of[shift][:, lanes])
            odd = ((row[:, 0:128] >> shift) & 1) == 1
            part = product_nt(jnp.where(odd, qh * weight, 0.0), jnp.where(odd, 0.0, kh * weight))
            scores = scores + jnp.where((row >> (shift + 1)) == (col >> (shift + 1)), part, 0.0)
        sh, sl = split2(scores)
        vh = vb[:, lanes]
        rec[h] = dot(sh, vh) + dot(sl, vh)

    take(st_recv, c_sem.at[0])
    cf = c.astype(f32)
    own, other = st_send[c], st_recv[c]
    first = own * (1.0 - cf) + other * cf
    second = other * (1.0 - cf) + own * cf
    chip_state = second[128:129, :] * first[0:128, :] + second[0:128, :]
    chip_decay = first[128:136, :] * second[128:136, :]
    for k in range(NX):
        tq[k, 0:32, :] = chip_state[32 * k : 32 * (k + 1), :]
        tq[k, 32:40, :] = chip_decay
    for dx in range(1, NX):
        to = (x + dx) % NX
        remote(tq.at[to], xr.at[x], s_sem.at[2], c_sem.at[1], {"sp_1": to}).start()
    xr[x] = tq[x]
    sums_of = {shift: sums(level_sum(shift)) for shift in (3, 4, 5, 6, 7)}
    take(xr.at[pl.ds(0, NX - 1)], c_sem.at[1])
    state, decay = jnp.zeros((32, 128), f32), jnp.ones((8, 128), f32)
    for k in range(NX):
        px[k, 0:32, :] = state
        px[k, 32:40, :] = decay
        state = xr[k, 32:33, :] * state + xr[k, 0:32, :]
        decay = xr[k, 32:40, :] * decay
    us[0:32, :] = state
    us[32:40, :] = decay
    for dz in (4, 3, 5, 2, 6, 1, 7):
        remote(us, zr.at[z], s_sem.at[3], c_sem.at[2], {"sp_0": (z + dz) % NZ}).start()
    zr[z] = us[...]
    inside(0)
    inside(1)
    take(zr.at[pl.ds(0, NZ - 1)], c_sem.at[2])
    state = jnp.zeros((32, 128), f32)
    for k in range(NZ):
        counts = (k < z).astype(f32)
        state = (1.0 - counts) * state + counts * (zr[k, 32:33, :] * state + zr[k, 0:32, :])
    for k in range(NX):
        isend[k] = px[k, 32:33, :] * state + px[k, 0:32, :]
    for dx in range(NX):
        to = (x + dx) % NX
        for dc in range(NC):
            if dx or dc:
                remote(
                    isend.at[to], inc.at[c * NX + x], s_sem.at[4], c_sem.at[3],
                    {"sp_1": to, "sp_2": (c + dc) % NC},
                ).start()
    inc[c * NX + x] = isend[x]
    take(inc.at[pl.ds(0, NX * NC - 1)], c_sem.at[3])

    loads[4].wait()
    for h in range(2):
        lanes = slice(128 * h, 128 * (h + 1))
        before = inc[NX * h : NX * (h + 1)].reshape(128, 128)
        before = (1.0 - cf) * before + cf * (
            st_recv[h, 128:129, :] * before + st_recv[h, 0:128, :]
        )
        recur = rec[h] + product_nt(qend[:, lanes], before)
        scale = lax.rsqrt(jnp.mean(recur * recur, axis=-1, keepdims=True) + EPS)
        gate_in = ob[:, lanes].astype(f32)
        gated = recur * scale * hg_ref[...] * (gate_in * jax.nn.sigmoid(gate_in))
        gall[p, :, lanes] = gated.astype(bf16)

    for half in range(2):
        rows = pl.ds(128 * half, 128)
        other = pl.ds(128 * (1 - half), 128)
        remote(gall.at[p, rows], gall.at[p, rows], s_sem.at[5], gm.at[half], at_up).start()
        remote(gall.at[p, other], gall.at[p, other], s_sem.at[5], gp.at[1 - half], at_down).start()
    low, high = pl.ds(0, 128), pl.ds(128, 128)
    loads[5].wait()

    def project(source, fresh):
        lhs = gall[source]
        for k in range(4):
            cols = slice(512 * k, 512 * (k + 1))
            part = dot(lhs, wh[source, :, cols])
            if fresh:
                acc[:, cols] = part
            else:
                acc[:, cols] = acc[:, cols] + part

    project(p, True)
    take(gall.at[down, low], gm.at[0])
    remote(gall.at[down, low], gall.at[down, low], s_sem.at[5], gr.at[0], at_up).start()
    take(gall.at[up, high], gp.at[1])
    remote(gall.at[up, high], gall.at[up, high], s_sem.at[5], gr.at[1], at_down).start()
    take(gall.at[down, high], gm.at[1])
    project(down, False)
    take(gall.at[up, low], gp.at[0])
    project(up, False)
    take(wd.at[down, low], wm.at[0])
    remote(wd.at[down, low], wd.at[down, low], s_sem.at[1], wr.at[0], at_up).start()
    take(wd.at[up, high], wp.at[1])
    remote(wd.at[up, high], wd.at[up, high], s_sem.at[1], wr.at[1], at_down).start()
    take(gall.at[far, low], gr.at[0])
    take(gall.at[far, high], gr.at[1])
    project(far, False)

    loads[6].wait()
    gain = fg_ref[...]

    def norm_rows(k, _):
        rows = pl.ds(pl.multiple_of(k * 32, 32), 32)
        wide = (stream[rows, :].astype(f32) + acc[rows, :]).astype(bf16)
        mixed[rows, :] = wide
        wide = wide.astype(f32)
        scale = lax.rsqrt(jnp.mean(wide * wide, axis=-1, keepdims=True) + EPS)
        done = (wide * scale * gain).astype(bf16)
        for quarter in range(4):
            normed[quarter, rows, :] = done[:, 512 * quarter : 512 * (quarter + 1)]
        return 0

    lax.fori_loop(0, ROWS // 32, norm_rows, 0)

    dest0, dest1 = dest_ref[0:1, :], dest_ref[1:2, :]
    slot = lax.broadcasted_iota(jnp.int32, (128, ROWS), 0)

    def dispatch(n, _):
        ids = slot + n * 128
        pick = jnp.where((ids == dest0) | (ids == dest1), 1.0, 0.0).astype(bf16)
        rows = dot(pick, normed[p]).astype(bf16).reshape(8, 16, 512)
        sbuf[pl.ds(n * 8, 8)] = rows
        dz = ring_step(n)
        for j in range(8):
            device = {
                "sp_0": (z + dz) % NZ, "sp_1": (x + j // 2) % NX, "sp_2": (c + j % 2) % NC,
            }

            def send(j=j, device=device):
                remote(
                    sbuf.at[n * 8 + j], xbuf.at[p, n * 8 + j], s_sem.at[6], xs.at[n], device
                ).start()

            if j:
                send()
            else:
                pl.when(n > 0)(send)

                @pl.when(n == 0)
                def _():
                    xbuf[p, 0] = rows[0]

        return 0

    lax.fori_loop(0, NZ, dispatch, 0)
    loads[7].wait()
    loads[8].wait()

    i0 = lax.broadcasted_iota(jnp.int32, (128, 128), 0)
    i1 = lax.broadcasted_iota(jnp.int32, (128, 128), 1)
    gather = ones_where(i1 == ((i0 >> 2) & 7) * 16 + (i0 >> 5) * 4 + (i0 & 3))
    spread = ones_where(i0 == ((i1 >> 2) & 7) * 16 + (i1 >> 5) * 4 + (i1 & 3))

    def stage_forward(n):
        group = pl.ds(n * 8, 8)

        @pl.when(n == 0)
        def _():
            take(xbuf.at[p, pl.ds(1, 7)], xs.at[n])

        @pl.when(n > 0)
        def _():
            take(xbuf.at[p, group], xs.at[n])

        remote(xbuf.at[p, group], xbuf.at[p, group], s_sem.at[7], yfm.at[n], at_up).start()
        remote(xbuf.at[p, group], xbuf.at[p, group], s_sem.at[7], yfp.at[n], at_down).start()

    def stage_relay(n):
        group = pl.ds(n * 8, 8)
        front, back = pl.ds(n * 8, 4), pl.ds(n * 8 + 4, 4)
        take(xbuf.at[down, group], yfm.at[n])
        remote(xbuf.at[down, front], xbuf.at[down, front], s_sem.at[7], yrm.at[n], at_up).start()
        take(xbuf.at[up, group], yfp.at[n])
        remote(xbuf.at[up, back], xbuf.at[up, back], s_sem.at[7], yrp.at[n], at_down).start()

    def stage_hidden(n):
        group = pl.ds(n * 8, 8)
        take(xbuf.at[far, pl.ds(n * 8, 4)], yrm.at[n])
        take(xbuf.at[far, pl.ds(n * 8 + 4, 4)], yrp.at[n])
        rows = jnp.concatenate([xbuf[k, group].reshape(128, 512) for k in range(NY)], axis=1)
        gate = dot(rows, wg[...])
        hidden = (gate * jax.nn.sigmoid(gate) * dot(rows, wu[...])).astype(bf16)
        hidden = dot(gather, hidden).astype(bf16).reshape(NY, 32, 256)
        hsend[n] = hidden
        for dy in range(1, NY):
            to = (p + dy) % NY
            remote(hsend.at[n, to], hrec.at[n, p], s_sem.at[8], hs.at[n], {"tp": to}).start()
        hrec[n, p] = hsend[n, p]

    def stage_down(n):
        take(hrec.at[n, pl.ds(0, NY - 1)], hs.at[n])
        rows = jnp.concatenate([hrec[n, k] for k in range(NY)], axis=1)
        outs = [
            dot(rows, wd[:, :, 512 * k : 512 * (k + 1)].reshape(1024, 512)).astype(bf16)
            for k in range(4)
        ]
        outs = dot(spread, jnp.concatenate(outs, axis=0)).astype(bf16).reshape(8, 16, 512)
        rsend[pl.ds(n * 8, 8)] = outs
        dz = ring_step(n)
        for j in range(8):
            device = {
                "sp_0": (z + NZ - dz) % NZ,
                "sp_1": (x + NX - j // 2) % NX,
                "sp_2": (c + j % 2) % NC,
            }

            def send(j=j, device=device):
                remote(
                    rsend.at[n * 8 + j], rbuf.at[n * 8 + j], s_sem.at[9], rs.at[n], device
                ).start()

            if j:
                send()
            else:
                pl.when(n > 0)(send)

                @pl.when(n == 0)
                def _():
                    rbuf[0] = outs[0]

    def pipeline(i, _):
        @pl.when(i < NZ)
        def _():
            stage_forward(i)

        @pl.when((i >= 1) & (i < NZ + 1))
        def _():
            stage_relay(i - 1)

        @pl.when((i >= 2) & (i < NZ + 2))
        def _():
            stage_hidden(i - 2)

        @pl.when(i == 3)
        def _():
            take(wd.at[down, high], wm.at[1])
            take(wd.at[up, low], wp.at[0])
            take(wd.at[far, low], wr.at[0])
            take(wd.at[far, high], wr.at[1])

        @pl.when(i >= 3)
        def _():
            stage_down(i - 3)

        return 0

    lax.fori_loop(0, NZ + 3, pipeline, 0)

    picks[...] = jnp.zeros_like(picks)
    base = base_ref[...]

    def combine(n, _):
        @pl.when(n == 0)
        def _():
            take(rbuf.at[pl.ds(1, 7)], rs.at[n])

        @pl.when(n > 0)
        def _():
            take(rbuf.at[pl.ds(n * 8, 8)], rs.at[n])

        rows = rbuf[pl.ds(n * 8, 8)].reshape(128, 512)
        for k in range(4):
            pick = jnp.where(i1 + (n * 128 - 4 * k) == base, 1.0, 0.0).astype(bf16)
            picks[k] = picks[k] + dot(pick, rows)
        return 0

    lax.fori_loop(0, NZ, combine, 0)
    own = mixed[pl.ds(pl.multiple_of(p * GROUP, GROUP), GROUP), :]
    for k in range(4):
        cols = slice(512 * k, 512 * (k + 1))
        routed = wsel_ref[:, 0:1] * picks[k, 0:64, :] + wsel_ref[:, 1:2] * picks[k, 64:128, :]
        out_ref[:, cols] = (own[:, cols].astype(f32) + routed).astype(bf16)

    take(st_send, s_sem.at[0])
    take(wd.at[pl.ds(0, 3)], s_sem.at[1])
    take(tq.at[pl.ds(0, 3)], s_sem.at[2])
    take(zr.at[pl.ds(0, 7)], s_sem.at[3])
    take(inc.at[pl.ds(0, 7)], s_sem.at[4])
    take(gall.at[pl.ds(0, 3)], s_sem.at[5])
    take(sbuf.at[pl.ds(0, 63)], s_sem.at[6])
    take(xbuf.at[pl.ds(0, 3)], s_sem.at[7])
    take(hrec.at[pl.ds(0, 6)], s_sem.at[8])
    take(rbuf.at[pl.ds(0, 63)], s_sem.at[9])


def per_device(
    stream, query, forget_gate_logits, value_input_rows, output_gate_logits, forget_floor_margin,
    additional_fading_speed, head_norm_gain, output_head_weight, feedforward_norm_gain,
    selected_expert_index, selected_expert_weight, expert_gate_weight, expert_up_weight,
    expert_down_weight,
):
    z, x, c, p = [lax.axis_index(name) for name in SP_TP]
    blocks = selected_expert_index.reshape(NY, GROUP * 2)
    same = blocks[:, :, None] == blocks[:, None, :]
    earlier = jnp.tril(jnp.ones((GROUP * 2, GROUP * 2), bool), -1)
    rank = jnp.sum((same & earlier).astype(jnp.int32), axis=2)
    dz = (blocks // 8 + NZ - z) % NZ
    group = jnp.where(dz <= 4, jnp.maximum(2 * dz - 1, 0), 2 * (NZ - dz))
    j = ((blocks // 2 % NX + NX - x) % NX) * 2 + (blocks % 2 + c) % NC
    start = (group * 8 + j) * 16 + rank
    dest = start + CAP * jnp.arange(NY, dtype=jnp.int32)[:, None]
    dest = dest.reshape(ROWS, 2).T
    base = lax.dynamic_index_in_dim(start, p, 0, keepdims=False).reshape(GROUP, 2)
    base = base.T.reshape(2 * GROUP, 1)

    vmem = pl.BlockSpec(memory_space=pltpu.VMEM)
    hbm = pl.BlockSpec(memory_space=pl.ANY)
    dma = pltpu.SemaphoreType.DMA
    V = pltpu.VMEM
    return pl.pallas_call(
        kernel,
        name="layer",
        out_shape=jax.ShapeDtypeStruct((GROUP, 2048), bf16),
        in_specs=[vmem] * 7 + [hbm] * 9,
        out_specs=vmem,
        scratch_shapes=[
            V((ROWS, 256), bf16), V((ROWS, 256), bf16), V((ROWS, 256), bf16), V((ROWS, 256), bf16),
            V((ROWS, 2048), bf16), V((4, 256, 2048), bf16), V((2048, 256), bf16),
            V((2048, 256), bf16), V((4, 256, 2048), bf16),
            V((2, ROWS, 128), f32), V((ROWS, 256), f32), V((2, 136, 128), f32),
            V((2, 136, 128), f32), V((4, 40, 128), f32), V((4, 40, 128), f32), V((4, 40, 128), f32),
            V((40, 128), f32), V((8, 40, 128), f32), V((4, 32, 128), f32), V((8, 32, 128), f32),
            V((4, ROWS, 256), bf16), V((ROWS, 2048), f32), V((ROWS, 2048), bf16),
            V((4, ROWS, 512), bf16), V((64, 16, 512), bf16), V((4, 64, 16, 512), bf16),
            V((8, 4, 32, 256), bf16), V((8, 4, 32, 256), bf16), V((64, 16, 512), bf16),
            V((64, 16, 512), bf16), V((4, 128, 512), f32),
            dma((9,)), dma((10,)), dma((4,)), dma((2,)), dma((2,)), dma((2,)), dma((2,)), dma((2,)),
            dma((2,)), dma((8,)), dma((8,)), dma((8,)), dma((8,)), dma((8,)), dma((8,)), dma((8,)),
        ],
        compiler_params=pltpu.CompilerParams(
            collective_id=0, has_side_effects=True, vmem_limit_bytes=60 * 1024 * 1024
        ),
    )(
        dest, base, selected_expert_weight, forget_floor_margin.reshape(1, 256),
        additional_fading_speed, head_norm_gain.reshape(1, 128),
        feedforward_norm_gain.reshape(1, 2048), query, forget_gate_logits, value_input_rows,
        output_gate_logits, stream, output_head_weight.reshape(4, 256, 2048), expert_gate_weight[0],
        expert_up_weight[0], expert_down_weight[0],
    )


def solution(mesh):
    finer = Mesh(mesh.devices.reshape(NZ, NX, NC, mesh.shape["tp"]), SP_TP)
    in_specs = (
        P(SP, None), P(SP, "tp"), P(SP, "tp"), P(SP, "tp"), P(SP, "tp"), P("tp", None),
        P(SP, "tp"), P(), P(), P(), P(SP, None), P(SP_TP, None), P(SP, None, "tp"),
        P(SP, None, "tp"), P(SP, "tp", None),
    )
    return jax.shard_map(
        per_device, mesh=finer, in_specs=in_specs, out_specs=P(SP_TP, None), check_vma=False
    )
```

```python
import functools

import jax
import jax.numpy as jnp
from jax import lax
from jax.experimental import pallas as pl
from jax.experimental.pallas import tpu as pltpu
from jax.sharding import Mesh
from jax.sharding import PartitionSpec as P

SP = ("sp_0", "sp_1", "sp_2")
SP_TP = ("sp_0", "sp_1", "sp_2", "tp")
EPS = 1e-06
f32 = jnp.float32
bf16 = jnp.bfloat16
NZ, NX, NC, NY = 8, 4, 2, 4
ROWS = 256
GROUP = 64
CAP = 4
NT = (((1,), (1,)), ((), ()))


def dot(a, b):
    return jnp.dot(a, b, preferred_element_type=f32)


def dot_nt(a, b):
    return lax.dot_general(a, b, NT, preferred_element_type=f32)


def split2(x):
    high = x.astype(bf16)
    return high, (x - high.astype(f32)).astype(bf16)


def split3(x):
    high = x.astype(bf16)
    rest = x - high.astype(f32)
    mid = rest.astype(bf16)
    return high, mid, (rest - mid.astype(f32)).astype(bf16)


def product_nt(a, b):
    ah, al = split2(a)
    bh, bl = split2(b)
    return dot_nt(jnp.concatenate([ah, ah, al], axis=1), jnp.concatenate([bh, bl, bh], axis=1))


ORDER = (0, 5, 4, 6, 3, 7, 2, 1)
PACKED = sum(dz << (3 * n) for n, dz in enumerate(ORDER))


def ring_step(n):
    return (PACKED >> (3 * n)) & 7


def remote(src, dst, send_sem, recv_sem, device):
    return pltpu.make_async_remote_copy(
        src_ref=src,
        dst_ref=dst,
        send_sem=send_sem,
        recv_sem=recv_sem,
        device_id=device,
        device_id_type=pl.DeviceIdType.MESH,
    )


def take(ref, sem):
    pltpu.make_async_copy(ref, ref, sem).wait()


def kernel(
    idx_ref, wsel_ref, mar_ref, fade_ref, hg_ref, fg_ref,
    q_hbm, f_hbm, v_hbm, og_hbm, stream_hbm, wh_hbm, wg_hbm, wu_hbm, wd_hbm,
    out_ref,
    qb, fb, vb, ob, stream, wh, wg, wu, wd,
    rec, qend, cs, cr, px, us, zr, isend, inc, dest, dcol,
    gall, acc, mixed, normed, sbuf, xbuf, hsend, hrec, rsend, rbuf, picks,
    load_sem, s_sem, c_sem, gm, gp, gr, wm, wp, wr, xs, yfm, yfp, yrm, yrp, hs, rs,
):
    z, x, c, p = [lax.axis_index(name) for name in SP_TP]
    up, down, far = (p + 1) % NY, (p + NY - 1) % NY, (p + 2) % NY
    at_up, at_down = {"tp": up}, {"tp": down}

    loads = [
        pltpu.make_async_copy(src, dst, load_sem.at[k])
        for k, (src, dst) in enumerate(
            [
                (f_hbm, fb), (q_hbm, qb), (v_hbm, vb), (wd_hbm, wd.at[p]), (og_hbm, ob),
                (wh_hbm, wh), (stream_hbm, stream), (wg_hbm, wg), (wu_hbm, wu),
            ]
        )
    ]
    for load in loads:
        load.start()

    barrier = pltpu.get_barrier_semaphore()

    def greet(k, _):
        dz, dx, dc = k // 8, (k // 2) % 4, k % 2
        pl.semaphore_signal(
            barrier,
            inc=1,
            device_id={"sp_0": (z + dz) % NZ, "sp_1": (x + dx) % NX, "sp_2": (c + dc) % NC},
            device_id_type=pl.DeviceIdType.MESH,
        )
        return 0

    for peer in (up, down, far):
        pl.semaphore_signal(
            barrier, inc=1, device_id={"tp": peer}, device_id_type=pl.DeviceIdType.MESH
        )
    lax.fori_loop(1, NZ * NX * NC, greet, 0)

    def as_column(line, width):
        return jnp.transpose(jnp.broadcast_to(line, (width, line.shape[1])), (1, 0))

    row = lax.broadcasted_iota(jnp.int32, (ROWS, ROWS), 0)
    col = lax.broadcasted_iota(jnp.int32, (ROWS, ROWS), 1)

    def ones_where(condition):
        return jnp.where(condition, 1.0, 0.0).astype(bf16)

    def level_sum(shift):
        odd = ((row >> shift) & 1) == 1
        same = (row >> shift) == (col >> shift)
        return ones_where(same & ((odd & (col <= row)) | (jnp.logical_not(odd) & (col > row))))

    def inside(h):
        lanes = slice(128 * h, 128 * (h + 1))
        qh, kh = queries[:, lanes], keys[:, lanes]
        exponent = sums_of[3][:, lanes]
        odd = ((row[:, 0:128] >> 3) & 1) == 1
        exponent = jnp.where(odd, exponent, -exponent)
        scores = product_nt(qh * jnp.exp(exponent), kh * jnp.exp(-exponent))
        scores = jnp.where(((row >> 4) == (col >> 4)) & (col <= row), scores, 0.0)
        for shift in (4, 5, 6, 7):
            weight = jnp.exp(sums_of[shift][:, lanes])
            odd = ((row[:, 0:128] >> shift) & 1) == 1
            part = product_nt(jnp.where(odd, qh * weight, 0.0), jnp.where(odd, 0.0, kh * weight))
            scores = scores + jnp.where((row >> (shift + 1)) == (col >> (shift + 1)), part, 0.0)
        sh, sl = split2(scores)
        vh = vb[:, lanes]
        rec[h] = dot(sh, vh) + dot(sl, vh)

    loads[0].wait()
    margin = jnp.concatenate([mar_ref[0:1, :], mar_ref[1:2, :]], axis=1)
    keys = margin * jax.nn.sigmoid(-fb[...].astype(f32))
    fades = jnp.concatenate([as_column(fade_ref[h : h + 1, :], 128) for h in range(2)], axis=1)
    log_decay = jnp.log1p(-keys) + fades
    parts = jnp.concatenate(split3(log_decay), axis=1)

    def sums(matrix):
        three = dot(matrix, parts)
        return three[:, 0:256] + (three[:, 256:512] + three[:, 512:768])

    loads[1].wait()
    loads[2].wait()
    queries = qb[...].astype(f32)
    to_start = sums(ones_where(col <= row))
    to_end = sums(ones_where(col > row))
    qend[...] = queries * jnp.exp(to_start)
    kend = keys * jnp.exp(to_end)
    total = jnp.exp(to_start[ROWS - 1 : ROWS, :])
    vt = jnp.transpose(vb[...].astype(f32), (1, 0)).astype(bf16)
    for h in range(2):
        lanes = slice(128 * h, 128 * (h + 1))
        kh, kl = split2(kend[:, lanes])
        both = dot(vt[lanes, :], jnp.concatenate([kh, kl], axis=1))
        both = both[:, 0:128] + both[:, 128:256]
        for k in range(NX):
            cs[k * NC + h, 0:32, :] = both[32 * k : 32 * (k + 1), :]
            cs[k * NC + h, 32:40, :] = jnp.broadcast_to(total[:, lanes], (8, 128))
    sums_of = {shift: sums(level_sum(shift)) for shift in (3, 4, 5, 6, 7)}
    inside(0)
    inside(1)

    chosen = [idx_ref[k : k + 1, :].astype(f32) for k in range(2)]
    columns = [as_column(e, ROWS) for e in chosen]
    block = (row >> 6) == (col >> 6)
    before = block & (row < col)

    def count(condition):
        return jnp.sum(jnp.where(condition, 1.0, 0.0), axis=0, keepdims=True)

    ranks = [
        count(before & (columns[0] == chosen[0])),
        count(block & (columns[0] == chosen[1])) + count(before & (columns[1] == chosen[1])),
    ]
    first_slot = CAP * (lax.broadcasted_iota(jnp.int32, (1, ROWS), 1) >> 6)
    for k in range(2):
        expert = idx_ref[k : k + 1, :]
        dz = ((expert >> 3) + NZ - z) & 7
        group = jnp.zeros_like(dz)
        for n, offset in enumerate(ORDER):
            group = jnp.where(dz == offset, n, group)
        j = (((expert >> 1) + NX - x) & 3) * 2 + ((expert + c) & 1)
        place = ((group * 8 + j) * 16 + first_slot).astype(f32) + ranks[k]
        dest[k : k + 1, :] = place
        dcol[k] = as_column(place, 128)

    pl.semaphore_wait(barrier, NZ * NX * NC - 1 + 3)

    def down_weights(n):
        rows, other = pl.ds(64 * n, 64), pl.ds(64 * (3 - n), 64)
        remote(wd.at[p, rows], wd.at[p, rows], s_sem.at[1], wm.at[n], at_up).start()
        remote(wd.at[p, other], wd.at[p, other], s_sem.at[1], wp.at[3 - n], at_down).start()

    for dx in (2, 1, 3, 0):
        to = (x + dx) % NX
        for dc in range(NC):
            if dx or dc:
                head = (c + dc) % NC
                remote(
                    cs.at[to * NC + head], cr.at[x * NC + c], s_sem.at[2], c_sem.at[1],
                    {"sp_1": to, "sp_2": head},
                ).start()
    loads[3].wait()
    down_weights(0)
    down_weights(1)
    cr[x * NC + c] = cs[x * NC + c]
    take(cr.at[pl.ds(0, NX * NC - 1)], c_sem.at[1])
    state, decay = jnp.zeros((32, 128), f32), jnp.ones((8, 128), f32)
    for k in range(NX * NC):
        px[k, 0:32, :] = state
        px[k, 32:40, :] = decay
        state = cr[k, 32:33, :] * state + cr[k, 0:32, :]
        decay = cr[k, 32:40, :] * decay
    us[0:32, :] = state
    us[32:40, :] = decay
    for dz in (4, 3, 5, 2, 6, 1, 7):
        remote(us, zr.at[z], s_sem.at[3], c_sem.at[2], {"sp_0": (z + dz) % NZ}).start()
    zr[z] = us[...]
    take(zr.at[pl.ds(0, NZ - 1)], c_sem.at[2])
    state = jnp.zeros((32, 128), f32)
    for k in range(NZ):
        counts = (k < z).astype(f32)
        state = (1.0 - counts) * state + counts * (zr[k, 32:33, :] * state + zr[k, 0:32, :])
    for k in range(NX * NC):
        isend[k] = px[k, 32:33, :] * state + px[k, 0:32, :]
    for dx in (2, 1, 3, 0):
        to = (x + dx) % NX
        for dc in range(NC):
            if dx or dc:
                core = (c + dc) % NC
                remote(
                    isend.at[to * NC + core], inc.at[c * NX + x], s_sem.at[4], c_sem.at[3],
                    {"sp_1": to, "sp_2": core},
                ).start()
    inc[c * NX + x] = isend[x * NC + c]
    take(inc.at[pl.ds(0, NX * NC - 1)], c_sem.at[3])

    loads[4].wait()
    for h in range(2):
        lanes = slice(128 * h, 128 * (h + 1))
        before = inc[NX * h : NX * (h + 1)].reshape(128, 128)
        recur = rec[h] + product_nt(qend[:, lanes], before)
        scale = lax.rsqrt(jnp.mean(recur * recur, axis=-1, keepdims=True) + EPS)
        gate_in = ob[:, lanes].astype(f32)
        gated = recur * scale * hg_ref[...] * (gate_in * jax.nn.sigmoid(gate_in))
        gall[p, :, lanes] = gated.astype(bf16)

    for half in range(2):
        rows = pl.ds(128 * half, 128)
        other = pl.ds(128 * (1 - half), 128)
        remote(gall.at[p, rows], gall.at[p, rows], s_sem.at[5], gm.at[half], at_up).start()
        remote(gall.at[p, other], gall.at[p, other], s_sem.at[5], gp.at[1 - half], at_down).start()
    low, high = pl.ds(0, 128), pl.ds(128, 128)
    loads[5].wait()

    def project(source, fresh):
        lhs = gall[source]
        for k in range(4):
            cols = slice(512 * k, 512 * (k + 1))
            part = dot(lhs, wh[source, :, cols])
            if fresh:
                acc[:, cols] = part
            else:
                acc[:, cols] = acc[:, cols] + part

    project(p, True)
    take(gall.at[down, low], gm.at[0])
    remote(gall.at[down, low], gall.at[down, low], s_sem.at[5], gr.at[0], at_up).start()
    take(gall.at[up, high], gp.at[1])
    remote(gall.at[up, high], gall.at[up, high], s_sem.at[5], gr.at[1], at_down).start()
    down_weights(2)
    for n in range(2):
        rows, other = pl.ds(64 * n, 64), pl.ds(64 * (3 - n), 64)
        take(wd.at[down, rows], wm.at[n])
        remote(wd.at[down, rows], wd.at[down, rows], s_sem.at[1], wr.at[n], at_up).start()
        take(wd.at[up, other], wp.at[3 - n])
        remote(wd.at[up, other], wd.at[up, other], s_sem.at[1], wr.at[3 - n], at_down).start()
    down_weights(3)
    take(gall.at[down, high], gm.at[1])
    project(down, False)
    take(gall.at[up, low], gp.at[0])
    project(up, False)
    take(gall.at[far, low], gr.at[0])
    take(gall.at[far, high], gr.at[1])
    project(far, False)

    loads[6].wait()
    gain = fg_ref[...]

    def norm_rows(k, _):
        rows = pl.ds(pl.multiple_of(k * 32, 32), 32)
        wide = (stream[rows, :].astype(f32) + acc[rows, :]).astype(bf16)
        mixed[rows, :] = wide
        wide = wide.astype(f32)
        scale = lax.rsqrt(jnp.mean(wide * wide, axis=-1, keepdims=True) + EPS)
        done = (wide * scale * gain).astype(bf16)
        for quarter in range(4):
            normed[quarter, rows, :] = done[:, 512 * quarter : 512 * (quarter + 1)]
        return 0

    lax.fori_loop(0, ROWS // 32, norm_rows, 0)

    dest0, dest1 = dest[0:1, :], dest[1:2, :]
    slot = lax.broadcasted_iota(jnp.int32, (128, ROWS), 0)

    def dispatch(n, _):
        ids = (slot + n * 128).astype(f32)
        pick = jnp.where((ids == dest0) | (ids == dest1), 1.0, 0.0).astype(bf16)
        rows = dot(pick, normed[p]).astype(bf16).reshape(8, 16, 512)
        sbuf[pl.ds(n * 8, 8)] = rows
        dz = ring_step(n)
        for j in range(8):
            device = {
                "sp_0": (z + dz) % NZ, "sp_1": (x + j // 2) % NX, "sp_2": (c + j % 2) % NC,
            }

            def send(j=j, device=device):
                remote(
                    sbuf.at[n * 8 + j], xbuf.at[p, n * 8 + j], s_sem.at[6], xs.at[n], device
                ).start()

            if j:
                send()
            else:
                pl.when(n > 0)(send)

                @pl.when(n == 0)
                def _():
                    xbuf[p, 0] = rows[0]


        return 0

    lax.fori_loop(0, NZ, dispatch, 0)
    loads[7].wait()
    loads[8].wait()

    i0 = lax.broadcasted_iota(jnp.int32, (128, 128), 0)
    i1 = lax.broadcasted_iota(jnp.int32, (128, 128), 1)
    gather = ones_where(i1 == ((i0 >> 2) & 7) * 16 + (i0 >> 5) * 4 + (i0 & 3))
    spread = ones_where(i0 == ((i1 >> 2) & 7) * 16 + (i1 >> 5) * 4 + (i1 & 3))

    def stage_forward(n):
        group = pl.ds(n * 8, 8)

        @pl.when(n == 0)
        def _():
            take(xbuf.at[p, pl.ds(1, 7)], xs.at[n])

        @pl.when(n > 0)
        def _():
            take(xbuf.at[p, group], xs.at[n])

        remote(xbuf.at[p, group], xbuf.at[p, group], s_sem.at[7], yfm.at[n], at_up).start()
        remote(xbuf.at[p, group], xbuf.at[p, group], s_sem.at[7], yfp.at[n], at_down).start()

    def stage_relay(n):
        group = pl.ds(n * 8, 8)
        front, back = pl.ds(n * 8, 3), pl.ds(n * 8 + 3, 5)
        take(xbuf.at[down, group], yfm.at[n])
        remote(xbuf.at[down, front], xbuf.at[down, front], s_sem.at[7], yrm.at[n], at_up).start()
        take(xbuf.at[up, group], yfp.at[n])
        remote(xbuf.at[up, back], xbuf.at[up, back], s_sem.at[7], yrp.at[n], at_down).start()

    def stage_hidden(n):
        group = pl.ds(n * 8, 8)
        take(xbuf.at[far, pl.ds(n * 8, 3)], yrm.at[n])
        take(xbuf.at[far, pl.ds(n * 8 + 3, 5)], yrp.at[n])
        rows = jnp.concatenate([xbuf[k, group].reshape(128, 512) for k in range(NY)], axis=1)
        gate = dot(rows, wg[...])
        hidden = (gate * jax.nn.sigmoid(gate) * dot(rows, wu[...])).astype(bf16)
        hidden = dot(gather, hidden).astype(bf16).reshape(NY, 32, 256)
        hsend[n] = hidden
        for dy in range(1, NY):
            to = (p + dy) % NY
            remote(hsend.at[n, to], hrec.at[n, p], s_sem.at[8], hs.at[n], {"tp": to}).start()
        hrec[n, p] = hsend[n, p]

    def stage_down(n):
        take(hrec.at[n, pl.ds(0, NY - 1)], hs.at[n])
        rows = jnp.concatenate([hrec[n, k] for k in range(NY)], axis=1)
        outs = [
            dot(rows, wd[:, :, 512 * k : 512 * (k + 1)].reshape(1024, 512)).astype(bf16)
            for k in range(4)
        ]
        outs = dot(spread, jnp.concatenate(outs, axis=0)).astype(bf16).reshape(8, 16, 512)
        rsend[pl.ds(n * 8, 8)] = outs
        dz = ring_step(n)
        for j in range(8):
            device = {
                "sp_0": (z + NZ - dz) % NZ,
                "sp_1": (x + NX - j // 2) % NX,
                "sp_2": (c + j % 2) % NC,
            }

            def send(j=j, device=device):
                remote(
                    rsend.at[n * 8 + j], rbuf.at[n * 8 + j], s_sem.at[9], rs.at[n], device
                ).start()

            if j:
                send()
            else:
                pl.when(n > 0)(send)

                @pl.when(n == 0)
                def _():
                    rbuf[0] = outs[0]


    def pipeline(i, _):
        @pl.when(i < NZ)
        def _():
            stage_forward(i)

        @pl.when((i >= 1) & (i < NZ + 1))
        def _():
            stage_relay(i - 1)

        @pl.when((i >= 2) & (i < NZ + 2))
        def _():
            stage_hidden(i - 2)

        @pl.when(i == 3)
        def _():
            for n in range(2):
                take(wd.at[down, pl.ds(64 * (n + 2), 64)], wm.at[n + 2])
                take(wd.at[up, pl.ds(64 * n, 64)], wp.at[n])
            for n in range(4):
                take(wd.at[far, pl.ds(64 * n, 64)], wr.at[n])

        @pl.when(i >= 3)
        def _():
            stage_down(i - 3)

        return 0

    lax.fori_loop(0, NZ + 3, pipeline, 0)

    picks[...] = jnp.zeros_like(picks)
    own_rows = pl.ds(pl.multiple_of(p * GROUP, GROUP), GROUP)
    base = jnp.concatenate([dcol[0, own_rows, :], dcol[1, own_rows, :]], axis=0)
    base = base - (CAP * p).astype(f32)

    def combine(n, _):
        @pl.when(n == 0)
        def _():
            take(rbuf.at[pl.ds(1, 7)], rs.at[n])

        @pl.when(n > 0)
        def _():
            take(rbuf.at[pl.ds(n * 8, 8)], rs.at[n])

        rows = rbuf[pl.ds(n * 8, 8)].reshape(128, 512)
        for k in range(4):
            pick = jnp.where((i1 + (n * 128 - 4 * k)).astype(f32) == base, 1.0, 0.0).astype(bf16)
            picks[k] = picks[k] + dot(pick, rows)
        return 0

    lax.fori_loop(0, NZ, combine, 0)
    own = mixed[own_rows, :]
    weight = as_column(jnp.concatenate([wsel_ref[0:1, :], wsel_ref[1:2, :]], axis=1), 128)
    for k in range(4):
        cols = slice(512 * k, 512 * (k + 1))
        weighted = weight[:, 0:1] * picks[k]
        routed = weighted[0:64, :] + weighted[64:128, :]
        out_ref[:, cols] = (own[:, cols].astype(f32) + routed).astype(bf16)

    take(wd.at[pl.ds(0, 3)], s_sem.at[1])
    take(cr.at[pl.ds(0, 7)], s_sem.at[2])
    take(zr.at[pl.ds(0, 7)], s_sem.at[3])
    take(inc.at[pl.ds(0, 7)], s_sem.at[4])
    take(gall.at[pl.ds(0, 3)], s_sem.at[5])
    take(sbuf.at[pl.ds(0, 63)], s_sem.at[6])
    take(xbuf.at[pl.ds(0, 3)], s_sem.at[7])
    take(hrec.at[pl.ds(0, 6)], s_sem.at[8])
    take(rbuf.at[pl.ds(0, 63)], s_sem.at[9])


def per_device(
    stream, query, forget_gate_logits, value_input_rows, output_gate_logits, forget_floor_margin,
    additional_fading_speed, head_norm_gain, output_head_weight, feedforward_norm_gain,
    selected_expert_index, selected_expert_weight, expert_gate_weight, expert_up_weight,
    expert_down_weight,
):
    vmem = pl.BlockSpec(memory_space=pltpu.VMEM)
    hbm = pl.BlockSpec(memory_space=pl.ANY)
    dma = pltpu.SemaphoreType.DMA
    V = pltpu.VMEM
    return pl.pallas_call(
        kernel,
        name="layer",
        out_shape=jax.ShapeDtypeStruct((GROUP, 2048), bf16),
        in_specs=[vmem] * 6 + [hbm] * 9,
        out_specs=vmem,
        scratch_shapes=[
            V((ROWS, 256), bf16), V((ROWS, 256), bf16), V((ROWS, 256), bf16), V((ROWS, 256), bf16),
            V((ROWS, 2048), bf16), V((4, 256, 2048), bf16), V((2048, 256), bf16),
            V((2048, 256), bf16), V((4, 256, 2048), bf16),
            V((2, ROWS, 128), f32), V((ROWS, 256), f32), V((8, 40, 128), f32), V((8, 40, 128), f32),
            V((8, 40, 128), f32), V((40, 128), f32), V((8, 40, 128), f32), V((8, 32, 128), f32),
            V((8, 32, 128), f32), V((2, ROWS), f32), V((2, ROWS, 128), f32),
            V((4, ROWS, 256), bf16), V((ROWS, 2048), f32), V((ROWS, 2048), bf16),
            V((4, ROWS, 512), bf16), V((64, 16, 512), bf16), V((4, 64, 16, 512), bf16),
            V((8, 4, 32, 256), bf16), V((8, 4, 32, 256), bf16), V((64, 16, 512), bf16),
            V((64, 16, 512), bf16), V((4, 128, 512), f32),
            dma((9,)), dma((10,)), dma((4,)), dma((2,)), dma((2,)), dma((2,)), dma((4,)), dma((4,)),
            dma((4,)), dma((8,)), dma((8,)), dma((8,)), dma((8,)), dma((8,)), dma((8,)), dma((8,)),
        ],
        compiler_params=pltpu.CompilerParams(
            collective_id=0, has_side_effects=True, vmem_limit_bytes=60 * 1024 * 1024
        ),
    )(
        selected_expert_index.T, selected_expert_weight.T, forget_floor_margin,
        additional_fading_speed.T, head_norm_gain.reshape(1, 128),
        feedforward_norm_gain.reshape(1, 2048), query, forget_gate_logits, value_input_rows,
        output_gate_logits, stream, output_head_weight.reshape(4, 256, 2048), expert_gate_weight[0],
        expert_up_weight[0], expert_down_weight[0],
    )


def solution(mesh):
    finer = Mesh(mesh.devices.reshape(NZ, NX, NC, mesh.shape["tp"]), SP_TP)
    in_specs = (
        P(SP, None), P(SP, "tp"), P(SP, "tp"), P(SP, "tp"), P(SP, "tp"), P("tp", None),
        P(SP, "tp"), P(), P(), P(), P(SP, None), P(SP_TP, None), P(SP, None, "tp"),
        P(SP, None, "tp"), P(SP, "tp", None),
    )
    return jax.shard_map(
        per_device, mesh=finer, in_specs=in_specs, out_specs=P(SP_TP, None), check_vma=False
    )
```

```python
import functools

import jax
import jax.numpy as jnp
from jax import lax
from jax.experimental import pallas as pl
from jax.experimental.pallas import tpu as pltpu
from jax.sharding import Mesh
from jax.sharding import PartitionSpec as P

SP = ("sp_0", "sp_1", "sp_2")
SP_TP = ("sp_0", "sp_1", "sp_2", "tp")
EPS = 1e-06
f32 = jnp.float32
bf16 = jnp.bfloat16
NZ, NX, NC, NY = 8, 4, 2, 4
ROWS = 256
GROUP = 64
CAP = 4
NT = (((1,), (1,)), ((), ()))


def dot(a, b):
    return jnp.dot(a, b, preferred_element_type=f32)


def dot_nt(a, b):
    return lax.dot_general(a, b, NT, preferred_element_type=f32)


def split2(x):
    high = x.astype(bf16)
    return high, (x - high.astype(f32)).astype(bf16)


def split3(x):
    high = x.astype(bf16)
    rest = x - high.astype(f32)
    mid = rest.astype(bf16)
    return high, mid, (rest - mid.astype(f32)).astype(bf16)


def product_nt(a, b):
    ah, al = split2(a)
    bh, bl = split2(b)
    return dot_nt(jnp.concatenate([ah, ah, al], axis=1), jnp.concatenate([bh, bl, bh], axis=1))


ORDER = (0, 4, 3, 5, 6, 2, 7, 1)
NEAR = 6
PACKED = sum(dz << (3 * n) for n, dz in enumerate(ORDER))


def ring_step(n):
    return (PACKED >> (3 * n)) & 7


def remote(src, dst, send_sem, recv_sem, device):
    return pltpu.make_async_remote_copy(
        src_ref=src,
        dst_ref=dst,
        send_sem=send_sem,
        recv_sem=recv_sem,
        device_id=device,
        device_id_type=pl.DeviceIdType.MESH,
    )


def take(ref, sem):
    pltpu.make_async_copy(ref, ref, sem).wait()


def kernel(
    idx_ref, wsel_ref, mar_ref, fade_ref, hg_ref, fg_ref,
    q_hbm, f_hbm, v_hbm, og_hbm, stream_hbm, wh_hbm, wg_hbm, wu_hbm, wd_hbm,
    out_ref,
    qb, fb, vb, ob, stream, wh, wg, wu, wd,
    rec, qend, cs, csd, cr, crd, px, pxd, us, usd, zr, zrd, isend, inc, dest, dcol,
    gall, acc, mixed, normed, sbuf, xbuf, hsend, hrec, rsend, rbuf, picks, sdir,
    load_sem, s_sem, c_sem, gm, gp, gr, wm, wp, wr, xs, yfm, yfp, yrm, yrp, hs, rs,
):
    z, x, c, p = [lax.axis_index(name) for name in SP_TP]
    up, down, far = (p + 1) % NY, (p + NY - 1) % NY, (p + 2) % NY
    at_up, at_down = {"tp": up}, {"tp": down}

    loads = [
        pltpu.make_async_copy(src, dst, load_sem.at[k])
        for k, (src, dst) in enumerate(
            [
                (f_hbm, fb), (q_hbm, qb), (v_hbm, vb), (wd_hbm, wd.at[p]), (og_hbm, ob),
                (wh_hbm, wh), (stream_hbm, stream), (wg_hbm, wg), (wu_hbm, wu),
            ]
        )
    ]
    for load in loads:
        load.start()

    barrier = pltpu.get_barrier_semaphore()

    def greet(dz, first):
        for k in range(first, NX * NC):
            pl.semaphore_signal(
                barrier,
                inc=1,
                device_id={
                    "sp_0": (z + dz) % NZ, "sp_1": (x + k // 2) % NX, "sp_2": (c + k % 2) % NC,
                },
                device_id_type=pl.DeviceIdType.MESH,
            )

    for peer in (up, down, far):
        pl.semaphore_signal(
            barrier, inc=1, device_id={"tp": peer}, device_id_type=pl.DeviceIdType.MESH
        )
    @pl.loop(1, NZ)
    def _(dz):
        greet(dz, 0)

    greet(0, 1)

    def as_column(line, width):
        return jnp.transpose(jnp.broadcast_to(line, (width, line.shape[1])), (1, 0))

    row = lax.broadcasted_iota(jnp.int32, (ROWS, ROWS), 0)
    col = lax.broadcasted_iota(jnp.int32, (ROWS, ROWS), 1)

    def ones_where(condition):
        return jnp.where(condition, 1.0, 0.0).astype(bf16)

    def level_sum(shift):
        odd = ((row >> shift) & 1) == 1
        same = (row >> shift) == (col >> shift)
        return ones_where(same & ((odd & (col <= row)) | (jnp.logical_not(odd) & (col > row))))

    def inside(h):
        lanes = slice(128 * h, 128 * (h + 1))
        qh, kh = queries[:, lanes], keys[:, lanes]
        exponent = sums_of[3][:, lanes]
        odd = ((row[:, 0:128] >> 3) & 1) == 1
        exponent = jnp.where(odd, exponent, -exponent)
        scores = product_nt(qh * jnp.exp(exponent), kh * jnp.exp(-exponent))
        scores = jnp.where(((row >> 4) == (col >> 4)) & (col <= row), scores, 0.0)
        for shift in (4, 5, 6, 7):
            weight = jnp.exp(sums_of[shift][:, lanes])
            odd = ((row[:, 0:128] >> shift) & 1) == 1
            part = product_nt(jnp.where(odd, qh * weight, 0.0), jnp.where(odd, 0.0, kh * weight))
            scores = scores + jnp.where((row >> (shift + 1)) == (col >> (shift + 1)), part, 0.0)
        sh, sl = split2(scores)
        vh = vb[:, lanes]
        rec[h] = dot(sh, vh) + dot(sl, vh)

    loads[0].wait()
    margin = jnp.concatenate([mar_ref[0:1, :], mar_ref[1:2, :]], axis=1)
    keys = margin * jax.nn.sigmoid(-fb[...].astype(f32))
    fades = jnp.concatenate([as_column(fade_ref[h : h + 1, :], 128) for h in range(2)], axis=1)
    log_decay = jnp.log1p(-keys) + fades
    parts = jnp.concatenate(split3(log_decay), axis=1)

    def sums(matrix):
        three = dot(matrix, parts)
        return three[:, 0:256] + (three[:, 256:512] + three[:, 512:768])

    loads[1].wait()
    loads[2].wait()
    queries = qb[...].astype(f32)
    to_start = sums(ones_where(col <= row))
    to_end = sums(ones_where(col > row))
    qend[...] = queries * jnp.exp(to_start)
    kend = keys * jnp.exp(to_end)
    total = jnp.exp(to_start[ROWS - 1 : ROWS, :])
    vt = jnp.transpose(vb[...].astype(f32), (1, 0)).astype(bf16)
    for h in range(2):
        lanes = slice(128 * h, 128 * (h + 1))
        kh, kl = split2(kend[:, lanes])
        both = dot(vt[lanes, :], jnp.concatenate([kh, kl], axis=1))
        both = both[:, 0:128] + both[:, 128:256]
        for k in range(NX):
            cs[k * NC + h] = both[32 * k : 32 * (k + 1), :]
            csd[k * NC + h] = total[:, lanes]
    sums_of = {shift: sums(level_sum(shift)) for shift in (3, 4, 5, 6, 7)}
    inside(0)
    inside(1)

    chosen = [idx_ref[k : k + 1, :].astype(f32) for k in range(2)]
    columns = [as_column(e, ROWS) for e in chosen]
    block = (row >> 6) == (col >> 6)
    before = block & (row < col)

    def count(condition):
        return jnp.sum(jnp.where(condition, 1.0, 0.0), axis=0, keepdims=True)

    ranks = [
        count(before & (columns[0] == chosen[0])),
        count(block & (columns[0] == chosen[1])) + count(before & (columns[1] == chosen[1])),
    ]
    first_slot = CAP * (lax.broadcasted_iota(jnp.int32, (1, ROWS), 1) >> 6)
    for k in range(2):
        expert = idx_ref[k : k + 1, :]
        dz = ((expert >> 3) + NZ - z) & 7
        group = jnp.zeros_like(dz)
        for n, offset in enumerate(ORDER):
            group = jnp.where(dz == offset, n, group)
        j = (((expert >> 1) + NX - x) & 3) * 2 + ((expert + c) & 1)
        place = ((group * 8 + j) * 16 + first_slot).astype(f32) + ranks[k]
        dest[k : k + 1, :] = place
        dcol[k] = as_column(place, 128)

    pl.semaphore_wait(barrier, NZ * NX * NC - 1 + 3)

    def down_weights(n):
        rows, other = pl.ds(32 * n, 32), pl.ds(32 * (7 - n), 32)
        remote(wd.at[p, rows], wd.at[p, rows], s_sem.at[1], wm.at[n], at_up).start()
        remote(wd.at[p, other], wd.at[p, other], s_sem.at[1], wp.at[7 - n], at_down).start()

    for dx in (2, 1, 3, 0):
        to = (x + dx) % NX
        for dc in range(NC):
            if dx or dc:
                head = (c + dc) % NC
                device = {"sp_1": to, "sp_2": head}
                remote(
                    cs.at[to * NC + head], cr.at[x * NC + c], s_sem.at[2], c_sem.at[1], device
                ).start()
                remote(
                    csd.at[to * NC + head], crd.at[x * NC + c], s_sem.at[10], c_sem.at[0], device
                ).start()
    loads[3].wait()
    for n in range(4):
        down_weights(n)
    cr[x * NC + c] = cs[x * NC + c]
    crd[x * NC + c] = csd[x * NC + c]
    take(cr.at[pl.ds(0, NX * NC - 1)], c_sem.at[1])
    take(crd.at[pl.ds(0, NX * NC - 1)], c_sem.at[0])
    state, decay = jnp.zeros((32, 128), f32), jnp.ones((1, 128), f32)
    for k in range(NX * NC):
        px[k] = state
        pxd[k] = decay
        state = crd[k] * state + cr[k]
        decay = crd[k] * decay
    us[...] = state
    usd[...] = decay
    for dz in (4, 3, 5, 2, 6, 1, 7):
        device = {"sp_0": (z + dz) % NZ}
        remote(us, zr.at[z], s_sem.at[3], c_sem.at[2], device).start()
        remote(usd, zrd.at[z], s_sem.at[11], c_sem.at[4], device).start()
    zr[z] = us[...]
    zrd[z] = usd[...]
    take(zr.at[pl.ds(0, NZ - 1)], c_sem.at[2])
    take(zrd.at[pl.ds(0, NZ - 1)], c_sem.at[4])
    state = jnp.zeros((32, 128), f32)
    for k in range(NZ):
        counts = (k < z).astype(f32)
        state = (1.0 - counts) * state + counts * (zrd[k] * state + zr[k])
    for k in range(NX * NC):
        isend[k] = pxd[k] * state + px[k]
    for dx in (2, 1, 3, 0):
        to = (x + dx) % NX
        for dc in range(NC):
            if dx or dc:
                core = (c + dc) % NC
                remote(
                    isend.at[to * NC + core], inc.at[c * NX + x], s_sem.at[4], c_sem.at[3],
                    {"sp_1": to, "sp_2": core},
                ).start()
    inc[c * NX + x] = isend[x * NC + c]
    down_weights(4)
    take(inc.at[pl.ds(0, NX * NC - 1)], c_sem.at[3])

    loads[4].wait()
    for h in range(2):
        lanes = slice(128 * h, 128 * (h + 1))
        before = inc[NX * h : NX * (h + 1)].reshape(128, 128)
        recur = rec[h] + product_nt(qend[:, lanes], before)
        scale = lax.rsqrt(jnp.mean(recur * recur, axis=-1, keepdims=True) + EPS)
        gate_in = ob[:, lanes].astype(f32)
        gated = recur * scale * hg_ref[...] * (gate_in * jax.nn.sigmoid(gate_in))
        gall[p, :, lanes] = gated.astype(bf16)

    for half in range(2):
        rows = pl.ds(128 * half, 128)
        other = pl.ds(128 * (1 - half), 128)
        remote(gall.at[p, rows], gall.at[p, rows], s_sem.at[5], gm.at[half], at_up).start()
        remote(gall.at[p, other], gall.at[p, other], s_sem.at[5], gp.at[1 - half], at_down).start()
    low, high = pl.ds(0, 128), pl.ds(128, 128)
    loads[5].wait()

    def project(source, fresh):
        lhs = gall[source]
        for k in range(4):
            cols = slice(512 * k, 512 * (k + 1))
            part = dot(lhs, wh[source, :, cols])
            if fresh:
                acc[:, cols] = part
            else:
                acc[:, cols] = acc[:, cols] + part

    project(p, True)
    take(gall.at[down, low], gm.at[0])
    remote(gall.at[down, low], gall.at[down, low], s_sem.at[5], gr.at[0], at_up).start()
    take(gall.at[up, high], gp.at[1])
    remote(gall.at[up, high], gall.at[up, high], s_sem.at[5], gr.at[1], at_down).start()
    down_weights(5)
    down_weights(6)
    for n in range(4):
        rows, other = pl.ds(32 * n, 32), pl.ds(32 * (7 - n), 32)
        take(wd.at[down, rows], wm.at[n])
        remote(wd.at[down, rows], wd.at[down, rows], s_sem.at[1], wr.at[n], at_up).start()
        take(wd.at[up, other], wp.at[7 - n])
        remote(wd.at[up, other], wd.at[up, other], s_sem.at[1], wr.at[7 - n], at_down).start()
    down_weights(7)
    take(gall.at[down, high], gm.at[1])
    project(down, False)
    take(gall.at[up, low], gp.at[0])
    project(up, False)
    take(gall.at[far, low], gr.at[0])
    take(gall.at[far, high], gr.at[1])
    project(far, False)

    loads[6].wait()
    gain = fg_ref[...]

    def norm_rows(k, _):
        rows = pl.ds(pl.multiple_of(k * 32, 32), 32)
        wide = (stream[rows, :].astype(f32) + acc[rows, :]).astype(bf16)
        mixed[rows, :] = wide
        wide = wide.astype(f32)
        scale = lax.rsqrt(jnp.mean(wide * wide, axis=-1, keepdims=True) + EPS)
        done = (wide * scale * gain).astype(bf16)
        for quarter in range(4):
            normed[quarter, rows, :] = done[:, 512 * quarter : 512 * (quarter + 1)]
        return 0

    lax.fori_loop(0, ROWS // 32, norm_rows, 0)

    dest0, dest1 = dest[0:1, :], dest[1:2, :]
    slot = lax.broadcasted_iota(jnp.int32, (128, ROWS), 0)

    def slots_of(n, quarter):
        ids = (slot + n * 128).astype(f32)
        pick = jnp.where((ids == dest0) | (ids == dest1), 1.0, 0.0).astype(bf16)
        return dot(pick, normed[quarter]).astype(bf16).reshape(8, 16, 512)

    def dispatch(n, _):
        sbuf[pl.ds(n * 8, 8)] = slots_of(n, p)
        dz = ring_step(n)
        for j in range(8):
            remote(
                sbuf.at[n * 8 + j], xbuf.at[p, n * 8 + j], s_sem.at[6], xs.at[n],
                {"sp_0": (z + dz) % NZ, "sp_1": (x + j // 2) % NX, "sp_2": (c + j % 2) % NC},
            ).start()
        return 0

    lax.fori_loop(1, NZ, dispatch, 0)
    def direct(k, n, quarter, sem):
        rows = slots_of(n, quarter)
        sdir[k] = rows
        for j in range(n == 0, 8):
            remote(
                sdir.at[k, j], xbuf.at[quarter, n * 8 + j], s_sem.at[0], sem,
                {
                    "sp_0": (z + ORDER[n]) % NZ,
                    "sp_1": (x + j // 2) % NX,
                    "sp_2": (c + j % 2) % NC,
                },
            ).start()
        return rows

    for quarter in range(NY):
        xbuf[quarter, 0] = direct(quarter, 0, quarter, xs.at[0])[0]
    for n in range(NEAR, NZ):
        direct(NY + n - NEAR, n, far, yrm.at[n])
    loads[7].wait()
    loads[8].wait()

    i0 = lax.broadcasted_iota(jnp.int32, (128, 128), 0)
    i1 = lax.broadcasted_iota(jnp.int32, (128, 128), 1)
    gather = ones_where(i1 == ((i0 >> 2) & 7) * 16 + (i0 >> 5) * 4 + (i0 & 3))
    spread = ones_where(i0 == ((i1 >> 2) & 7) * 16 + (i1 >> 5) * 4 + (i1 & 3))

    def stage_forward(n):
        group = pl.ds(n * 8, 8)

        take(xbuf.at[p, group], xs.at[n])
        remote(xbuf.at[p, group], xbuf.at[p, group], s_sem.at[7], yfm.at[n], at_up).start()
        remote(xbuf.at[p, group], xbuf.at[p, group], s_sem.at[7], yfp.at[n], at_down).start()

    def stage_relay(n):
        group = pl.ds(n * 8, 8)
        front, back = pl.ds(n * 8, 4), pl.ds(n * 8 + 4, 4)
        take(xbuf.at[down, group], yfm.at[n])

        @pl.when(n < NEAR)
        def _():
            remote(xbuf.at[down, front], xbuf.at[down, front], s_sem.at[7], yrm.at[n], at_up).start()

        take(xbuf.at[up, group], yfp.at[n])

        @pl.when(n < NEAR)
        def _():
            remote(xbuf.at[up, back], xbuf.at[up, back], s_sem.at[7], yrp.at[n], at_down).start()


    def stage_hidden(n):
        group = pl.ds(n * 8, 8)
        @pl.when(n == 0)
        def _():
            take(xbuf.at[0, pl.ds(0, 28)], xs.at[0])

        @pl.when(n >= NEAR)
        def _():
            take(xbuf.at[far, group], yrm.at[n])

        @pl.when((n > 0) & (n < NEAR))
        def _():
            take(xbuf.at[far, pl.ds(n * 8, 4)], yrm.at[n])
            take(xbuf.at[far, pl.ds(n * 8 + 4, 4)], yrp.at[n])

        rows = jnp.concatenate([xbuf[k, group].reshape(128, 512) for k in range(NY)], axis=1)
        gate = dot(rows, wg[...])
        hidden = (gate * jax.nn.sigmoid(gate) * dot(rows, wu[...])).astype(bf16)
        hidden = dot(gather, hidden).astype(bf16).reshape(NY, 32, 256)
        hsend[n] = hidden
        for dy in range(1, NY):
            to = (p + dy) % NY
            remote(hsend.at[n, to], hrec.at[n, p], s_sem.at[8], hs.at[n], {"tp": to}).start()
        hrec[n, p] = hsend[n, p]

    def stage_down(n):
        take(hrec.at[n, pl.ds(0, NY - 1)], hs.at[n])
        rows = jnp.concatenate([hrec[n, k] for k in range(NY)], axis=1)
        outs = [
            dot(rows, wd[:, :, 512 * k : 512 * (k + 1)].reshape(1024, 512)).astype(bf16)
            for k in range(4)
        ]
        outs = dot(spread, jnp.concatenate(outs, axis=0)).astype(bf16).reshape(8, 16, 512)
        rsend[pl.ds(n * 8, 8)] = outs
        dz = ring_step(n)
        for j in range(8):
            device = {
                "sp_0": (z + NZ - dz) % NZ,
                "sp_1": (x + NX - j // 2) % NX,
                "sp_2": (c + j % 2) % NC,
            }

            def send(j=j, device=device):
                remote(
                    rsend.at[n * 8 + j], rbuf.at[n * 8 + j], s_sem.at[9], rs.at[n], device
                ).start()

            if j:
                send()
            else:
                pl.when(n > 0)(send)

                @pl.when(n == 0)
                def _():
                    rbuf[0] = outs[0]


    @pl.loop(1, NZ + 3)
    def _(i):
        @pl.when(i < NZ)
        def _():
            stage_forward(i)

        @pl.when((i >= 2) & (i < NZ + 1))
        def _():
            stage_relay(i - 1)

        @pl.when((i >= 2) & (i < NZ + 2))
        def _():
            stage_hidden(i - 2)

        @pl.when(i == 3)
        def _():
            for n in range(4):
                take(wd.at[down, pl.ds(32 * (n + 4), 32)], wm.at[n + 4])
                take(wd.at[up, pl.ds(32 * n, 32)], wp.at[n])
            for n in range(8):
                take(wd.at[far, pl.ds(32 * n, 32)], wr.at[n])

        @pl.when(i >= 3)
        def _():
            stage_down(i - 3)

    picks[...] = jnp.zeros_like(picks)
    own_rows = pl.ds(pl.multiple_of(p * GROUP, GROUP), GROUP)
    base = jnp.concatenate([dcol[0, own_rows, :], dcol[1, own_rows, :]], axis=0)
    base = base - (CAP * p).astype(f32)

    def combine(n, _):
        @pl.when(n == 0)
        def _():
            take(rbuf.at[pl.ds(1, 7)], rs.at[n])

        @pl.when(n > 0)
        def _():
            take(rbuf.at[pl.ds(n * 8, 8)], rs.at[n])

        rows = rbuf[pl.ds(n * 8, 8)].reshape(128, 512)
        for k in range(4):
            pick = jnp.where((i1 + (n * 128 - 4 * k)).astype(f32) == base, 1.0, 0.0).astype(bf16)
            picks[k] = picks[k] + dot(pick, rows)
        return 0

    lax.fori_loop(0, NZ, combine, 0)
    own = mixed[own_rows, :]
    weight = as_column(jnp.concatenate([wsel_ref[0:1, :], wsel_ref[1:2, :]], axis=1), 128)
    for k in range(4):
        cols = slice(512 * k, 512 * (k + 1))
        weighted = weight[:, 0:1] * picks[k]
        routed = weighted[0:64, :] + weighted[64:128, :]
        out_ref[:, cols] = (own[:, cols].astype(f32) + routed).astype(bf16)

    take(wd.at[pl.ds(0, 3)], s_sem.at[1])
    take(cr.at[pl.ds(0, 7)], s_sem.at[2])
    take(crd.at[pl.ds(0, 7)], s_sem.at[10])
    take(zr.at[pl.ds(0, 7)], s_sem.at[3])
    take(zrd.at[pl.ds(0, 7)], s_sem.at[11])
    take(inc.at[pl.ds(0, 7)], s_sem.at[4])
    take(gall.at[pl.ds(0, 3)], s_sem.at[5])
    take(xbuf.at[0, pl.ds(0, 28)], s_sem.at[0])
    take(xbuf.at[0, pl.ds(0, 8 * (NZ - NEAR))], s_sem.at[0])
    take(sbuf.at[pl.ds(0, 56)], s_sem.at[6])
    for k in range(2):
        take(xbuf.at[k, pl.ds(0, 8 * (NZ - 1))], s_sem.at[7])
    take(xbuf.at[2, pl.ds(0, 8 * (NEAR - 1))], s_sem.at[7])
    take(hrec.at[pl.ds(0, 6)], s_sem.at[8])
    take(rbuf.at[pl.ds(0, 63)], s_sem.at[9])


def per_device(
    stream, query, forget_gate_logits, value_input_rows, output_gate_logits, forget_floor_margin,
    additional_fading_speed, head_norm_gain, output_head_weight, feedforward_norm_gain,
    selected_expert_index, selected_expert_weight, expert_gate_weight, expert_up_weight,
    expert_down_weight,
):
    vmem = pl.BlockSpec(memory_space=pltpu.VMEM)
    hbm = pl.BlockSpec(memory_space=pl.ANY)
    dma = pltpu.SemaphoreType.DMA
    V = pltpu.VMEM
    return pl.pallas_call(
        kernel,
        name="layer",
        out_shape=jax.ShapeDtypeStruct((GROUP, 2048), bf16),
        in_specs=[vmem] * 6 + [hbm] * 9,
        out_specs=vmem,
        scratch_shapes=[
            V((ROWS, 256), bf16), V((ROWS, 256), bf16), V((ROWS, 256), bf16), V((ROWS, 256), bf16),
            V((ROWS, 2048), bf16), V((4, 256, 2048), bf16), V((2048, 256), bf16),
            V((2048, 256), bf16), V((4, 256, 2048), bf16),
            V((2, ROWS, 128), f32), V((ROWS, 256), f32), V((8, 32, 128), f32), V((8, 1, 128), f32),
            V((8, 32, 128), f32), V((8, 1, 128), f32), V((8, 32, 128), f32), V((8, 1, 128), f32),
            V((32, 128), f32), V((1, 128), f32), V((8, 32, 128), f32), V((8, 1, 128), f32),
            V((8, 32, 128), f32), V((8, 32, 128), f32), V((2, ROWS), f32), V((2, ROWS, 128), f32),
            V((4, ROWS, 256), bf16), V((ROWS, 2048), f32), V((ROWS, 2048), bf16),
            V((4, ROWS, 512), bf16), V((64, 16, 512), bf16), V((4, 64, 16, 512), bf16),
            V((8, 4, 32, 256), bf16), V((8, 4, 32, 256), bf16), V((64, 16, 512), bf16),
            V((64, 16, 512), bf16), V((4, 128, 512), f32), V((6, 8, 16, 512), bf16),
            dma((9,)), dma((12,)), dma((5,)), dma((2,)), dma((2,)), dma((2,)), dma((8,)), dma((8,)),
            dma((8,)), dma((8,)), dma((8,)), dma((8,)), dma((8,)), dma((8,)), dma((8,)), dma((8,)),
        ],
        compiler_params=pltpu.CompilerParams(
            collective_id=0, has_side_effects=True, vmem_limit_bytes=60 * 1024 * 1024
        ),
    )(
        selected_expert_index.T, selected_expert_weight.T, forget_floor_margin,
        additional_fading_speed.T, head_norm_gain.reshape(1, 128),
        feedforward_norm_gain.reshape(1, 2048), query, forget_gate_logits, value_input_rows,
        output_gate_logits, stream, output_head_weight.reshape(4, 256, 2048), expert_gate_weight[0],
        expert_up_weight[0], expert_down_weight[0],
    )


def solution(mesh):
    finer = Mesh(mesh.devices.reshape(NZ, NX, NC, mesh.shape["tp"]), SP_TP)
    in_specs = (
        P(SP, None), P(SP, "tp"), P(SP, "tp"), P(SP, "tp"), P(SP, "tp"), P("tp", None),
        P(SP, "tp"), P(), P(), P(), P(SP, None), P(SP_TP, None), P(SP, None, "tp"),
        P(SP, None, "tp"), P(SP, "tp", None),
    )
    return jax.shard_map(
        per_device, mesh=finer, in_specs=in_specs, out_specs=P(SP_TP, None), check_vma=False
    )
```

```python
import functools

import jax
import jax.numpy as jnp
from jax import lax
from jax.experimental import pallas as pl
from jax.experimental.pallas import tpu as pltpu
from jax.sharding import Mesh
from jax.sharding import PartitionSpec as P

SP = ("sp_0", "sp_1", "sp_2")
SP_TP = ("sp_0", "sp_1", "sp_2", "tp")
EPS = 1e-06
f32 = jnp.float32
bf16 = jnp.bfloat16
NZ, NX, NC, NY = 8, 4, 2, 4
ROWS = 256
GROUP = 64
CAP = 4
NT = (((1,), (1,)), ((), ()))


def dot(a, b):
    return jnp.dot(a, b, preferred_element_type=f32)


def dot_nt(a, b):
    return lax.dot_general(a, b, NT, preferred_element_type=f32)


def split2(x):
    high = x.astype(bf16)
    return high, (x - high.astype(f32)).astype(bf16)


def split3(x):
    high = x.astype(bf16)
    rest = x - high.astype(f32)
    mid = rest.astype(bf16)
    return high, mid, (rest - mid.astype(f32)).astype(bf16)


def product_nt(a, b):
    ah, al = split2(a)
    bh, bl = split2(b)
    return dot_nt(jnp.concatenate([ah, ah, al], axis=1), jnp.concatenate([bh, bl, bh], axis=1))


ORDER = (0, 4, 3, 5, 6, 2, 7, 1)
NEAR = 4
PACKED = sum(dz << (3 * n) for n, dz in enumerate(ORDER))


def ring_step(n):
    return (PACKED >> (3 * n)) & 7


def remote(src, dst, send_sem, recv_sem, device):
    return pltpu.make_async_remote_copy(
        src_ref=src,
        dst_ref=dst,
        send_sem=send_sem,
        recv_sem=recv_sem,
        device_id=device,
        device_id_type=pl.DeviceIdType.MESH,
    )


def take(ref, sem):
    pltpu.make_async_copy(ref, ref, sem).wait()


def kernel(
    idx_ref, wsel_ref, mar_ref, fade_ref, hg_ref, fg_ref,
    q_hbm, f_hbm, v_hbm, og_hbm, stream_hbm, wh_hbm, wg_hbm, wu_hbm, wd_hbm,
    out_ref,
    qb, fb, vb, ob, stream, wh, wg, wu, wd,
    rec, qend, cs, csd, cr, crd, px, pxd, us, usd, zr, zrd, isend, inc, dest, dcol,
    gall, acc, mixed, normed, sbuf, xbuf, hsend, hrec, rsend, rbuf, picks, sdir,
    load_sem, s_sem, c_sem, g_sem, wm, wp, wr, xs, yfm, yfp, yrm, yrp, hs, rs,
):
    z, x, c, p = [lax.axis_index(name) for name in SP_TP]
    up, down, far = (p + 1) % NY, (p + NY - 1) % NY, (p + 2) % NY
    at_up, at_down = {"tp": up}, {"tp": down}

    loads = [
        pltpu.make_async_copy(src, dst, load_sem.at[k])
        for k, (src, dst) in enumerate(
            [
                (f_hbm, fb), (q_hbm, qb), (v_hbm, vb), (wd_hbm, wd.at[p]), (og_hbm, ob),
                (wh_hbm, wh), (stream_hbm, stream), (wg_hbm, wg), (wu_hbm, wu),
            ]
        )
    ]
    for load in loads:
        load.start()

    barrier = pltpu.get_barrier_semaphore()

    def greet(dz, first):
        for k in range(first, NX * NC):
            pl.semaphore_signal(
                barrier,
                inc=1,
                device_id={
                    "sp_0": (z + dz) % NZ, "sp_1": (x + k // 2) % NX, "sp_2": (c + k % 2) % NC,
                },
                device_id_type=pl.DeviceIdType.MESH,
            )

    for peer in (up, down, far):
        pl.semaphore_signal(
            barrier, inc=1, device_id={"tp": peer}, device_id_type=pl.DeviceIdType.MESH
        )
    @pl.loop(1, NZ)
    def _(dz):
        greet(dz, 0)

    greet(0, 1)

    def as_column(line, width):
        return jnp.transpose(jnp.broadcast_to(line, (width, line.shape[1])), (1, 0))

    row = lax.broadcasted_iota(jnp.int32, (ROWS, ROWS), 0)
    col = lax.broadcasted_iota(jnp.int32, (ROWS, ROWS), 1)

    def ones_where(condition):
        return jnp.where(condition, 1.0, 0.0).astype(bf16)

    def level_sum(shift):
        odd = ((row >> shift) & 1) == 1
        same = (row >> shift) == (col >> shift)
        return ones_where(same & ((odd & (col <= row)) | (jnp.logical_not(odd) & (col > row))))

    def inside(h):
        lanes = slice(128 * h, 128 * (h + 1))
        qh, kh = queries[:, lanes], keys[:, lanes]
        exponent = sums_of[3][:, lanes]
        odd = ((row[:, 0:128] >> 3) & 1) == 1
        exponent = jnp.where(odd, exponent, -exponent)
        scores = product_nt(qh * jnp.exp(exponent), kh * jnp.exp(-exponent))
        scores = jnp.where(((row >> 4) == (col >> 4)) & (col <= row), scores, 0.0)
        for shift in (4, 5, 6, 7):
            weight = jnp.exp(sums_of[shift][:, lanes])
            odd = ((row[:, 0:128] >> shift) & 1) == 1
            part = product_nt(jnp.where(odd, qh * weight, 0.0), jnp.where(odd, 0.0, kh * weight))
            scores = scores + jnp.where((row >> (shift + 1)) == (col >> (shift + 1)), part, 0.0)
        sh, sl = split2(scores)
        vh = vb[:, lanes]
        rec[h] = dot(sh, vh) + dot(sl, vh)

    loads[0].wait()
    margin = jnp.concatenate([mar_ref[0:1, :], mar_ref[1:2, :]], axis=1)
    keys = margin * jax.nn.sigmoid(-fb[...].astype(f32))
    fades = jnp.concatenate([as_column(fade_ref[h : h + 1, :], 128) for h in range(2)], axis=1)
    log_decay = jnp.log1p(-keys) + fades
    parts = jnp.concatenate(split3(log_decay), axis=1)

    def sums(matrix):
        three = dot(matrix, parts)
        return three[:, 0:256] + (three[:, 256:512] + three[:, 512:768])

    loads[1].wait()
    loads[2].wait()
    queries = qb[...].astype(f32)
    to_start = sums(ones_where(col <= row))
    to_end = sums(ones_where(col > row))
    qend[...] = queries * jnp.exp(to_start)
    kend = keys * jnp.exp(to_end)
    total = jnp.exp(to_start[ROWS - 1 : ROWS, :])
    vt = jnp.transpose(vb[...].astype(f32), (1, 0)).astype(bf16)
    for h in range(2):
        lanes = slice(128 * h, 128 * (h + 1))
        kh, kl = split2(kend[:, lanes])
        both = dot(vt[lanes, :], jnp.concatenate([kh, kl], axis=1))
        both = both[:, 0:128] + both[:, 128:256]
        for k in range(NX):
            cs[k * NC + h] = both[32 * k : 32 * (k + 1), :]
            csd[k * NC + h] = total[:, lanes]
    sums_of = {shift: sums(level_sum(shift)) for shift in (3, 4, 5, 6, 7)}
    inside(0)
    inside(1)

    chosen = [idx_ref[k : k + 1, :].astype(f32) for k in range(2)]
    columns = [as_column(e, ROWS) for e in chosen]
    block = (row >> 6) == (col >> 6)
    before = block & (row < col)

    def count(condition):
        return jnp.sum(jnp.where(condition, 1.0, 0.0), axis=0, keepdims=True)

    ranks = [
        count(before & (columns[0] == chosen[0])),
        count(block & (columns[0] == chosen[1])) + count(before & (columns[1] == chosen[1])),
    ]
    first_slot = CAP * (lax.broadcasted_iota(jnp.int32, (1, ROWS), 1) >> 6)
    for k in range(2):
        expert = idx_ref[k : k + 1, :]
        dz = ((expert >> 3) + NZ - z) & 7
        group = jnp.zeros_like(dz)
        for n, offset in enumerate(ORDER):
            group = jnp.where(dz == offset, n, group)
        j = (((expert >> 1) + NX - x) & 3) * 2 + ((expert + c) & 1)
        place = ((group * 8 + j) * 16 + first_slot).astype(f32) + ranks[k]
        dest[k : k + 1, :] = place
        dcol[k] = as_column(place, 128)

    pl.semaphore_wait(barrier, NZ * NX * NC - 1 + 3)

    def down_weights(n):
        rows, other = pl.ds(32 * n, 32), pl.ds(32 * (7 - n), 32)
        remote(wd.at[p, rows], wd.at[p, rows], s_sem.at[1], wm.at[n], at_up).start()
        remote(wd.at[p, other], wd.at[p, other], s_sem.at[1], wp.at[7 - n], at_down).start()

    for dx in (2, 1, 3, 0):
        to = (x + dx) % NX
        for dc in range(NC):
            if dx or dc:
                head = (c + dc) % NC
                device = {"sp_1": to, "sp_2": head}
                remote(
                    cs.at[to * NC + head], cr.at[x * NC + c], s_sem.at[2], c_sem.at[1], device
                ).start()
                remote(
                    csd.at[to * NC + head], crd.at[x * NC + c], s_sem.at[10], c_sem.at[0], device
                ).start()
    loads[3].wait()
    for n in range(4):
        down_weights(n)
    cr[x * NC + c] = cs[x * NC + c]
    crd[x * NC + c] = csd[x * NC + c]
    take(cr.at[pl.ds(0, NX * NC - 1)], c_sem.at[1])
    take(crd.at[pl.ds(0, NX * NC - 1)], c_sem.at[0])
    state, decay = jnp.zeros((32, 128), f32), jnp.ones((1, 128), f32)
    for k in range(NX * NC):
        px[k] = state
        pxd[k] = decay
        state = crd[k] * state + cr[k]
        decay = crd[k] * decay
    us[...] = state
    usd[...] = decay
    for dz in (4, 3, 5, 2, 6, 1, 7):
        device = {"sp_0": (z + dz) % NZ}
        remote(us, zr.at[z], s_sem.at[3], c_sem.at[2], device).start()
        remote(usd, zrd.at[z], s_sem.at[11], c_sem.at[4], device).start()
    zr[z] = us[...]
    zrd[z] = usd[...]
    take(zr.at[pl.ds(0, NZ - 1)], c_sem.at[2])
    take(zrd.at[pl.ds(0, NZ - 1)], c_sem.at[4])
    state = jnp.zeros((32, 128), f32)
    for k in range(NZ):
        counts = (k < z).astype(f32)
        state = (1.0 - counts) * state + counts * (zrd[k] * state + zr[k])
    for k in range(NX * NC):
        isend[k] = pxd[k] * state + px[k]
    for dx in (2, 1, 3, 0):
        to = (x + dx) % NX
        for dc in range(NC):
            if dx or dc:
                core = (c + dc) % NC
                remote(
                    isend.at[to * NC + core], inc.at[c * NX + x], s_sem.at[4], c_sem.at[3],
                    {"sp_1": to, "sp_2": core},
                ).start()
    inc[c * NX + x] = isend[x * NC + c]
    down_weights(4)
    take(inc.at[pl.ds(0, NX * NC - 1)], c_sem.at[3])

    loads[4].wait()
    for h in range(2):
        lanes = slice(128 * h, 128 * (h + 1))
        before = inc[NX * h : NX * (h + 1)].reshape(128, 128)
        recur = rec[h] + product_nt(qend[:, lanes], before)
        scale = lax.rsqrt(jnp.mean(recur * recur, axis=-1, keepdims=True) + EPS)
        gate_in = ob[:, lanes].astype(f32)
        gated = recur * scale * hg_ref[...] * (gate_in * jax.nn.sigmoid(gate_in))
        gall[p, :, lanes] = gated.astype(bf16)

    for k, peer in enumerate((up, down, far)):
        remote(gall.at[p], gall.at[p], s_sem.at[5], g_sem.at[k], {"tp": peer}).start()
    for n in range(5, 8):
        down_weights(n)
    loads[5].wait()

    def project(source, fresh):
        lhs = gall[source]
        for k in range(4):
            cols = slice(512 * k, 512 * (k + 1))
            part = dot(lhs, wh[source, :, cols])
            if fresh:
                acc[:, cols] = part
            else:
                acc[:, cols] = acc[:, cols] + part

    project(p, True)
    take(gall.at[down], g_sem.at[0])
    for n in range(4):
        rows, other = pl.ds(32 * n, 32), pl.ds(32 * (7 - n), 32)
        take(wd.at[down, rows], wm.at[n])
        remote(wd.at[down, rows], wd.at[down, rows], s_sem.at[1], wr.at[n], at_up).start()
        take(wd.at[up, other], wp.at[7 - n])
        remote(wd.at[up, other], wd.at[up, other], s_sem.at[1], wr.at[7 - n], at_down).start()
    project(down, False)
    take(gall.at[up], g_sem.at[1])
    project(up, False)
    take(gall.at[far], g_sem.at[2])
    project(far, False)

    loads[6].wait()
    gain = fg_ref[...]

    def norm_rows(k, _):
        rows = pl.ds(pl.multiple_of(k * 32, 32), 32)
        wide = (stream[rows, :].astype(f32) + acc[rows, :]).astype(bf16)
        mixed[rows, :] = wide
        wide = wide.astype(f32)
        scale = lax.rsqrt(jnp.mean(wide * wide, axis=-1, keepdims=True) + EPS)
        done = (wide * scale * gain).astype(bf16)
        for quarter in range(4):
            normed[quarter, rows, :] = done[:, 512 * quarter : 512 * (quarter + 1)]
        return 0

    lax.fori_loop(0, ROWS // 32, norm_rows, 0)

    dest0, dest1 = dest[0:1, :], dest[1:2, :]
    slot = lax.broadcasted_iota(jnp.int32, (128, ROWS), 0)

    def slots_of(n, quarter):
        ids = (slot + n * 128).astype(f32)
        pick = jnp.where((ids == dest0) | (ids == dest1), 1.0, 0.0).astype(bf16)
        return dot(pick, normed[quarter]).astype(bf16).reshape(8, 16, 512)

    def dispatch(n, _):
        sbuf[pl.ds(n * 8, 8)] = slots_of(n, p)
        dz = ring_step(n)
        for j in range(8):
            remote(
                sbuf.at[n * 8 + j], xbuf.at[p, n * 8 + j], s_sem.at[6], xs.at[n],
                {"sp_0": (z + dz) % NZ, "sp_1": (x + j // 2) % NX, "sp_2": (c + j % 2) % NC},
            ).start()
        return 0

    lax.fori_loop(1, NZ, dispatch, 0)
    def direct(k, n, quarter, sem):
        rows = slots_of(n, quarter)
        sdir[k] = rows
        for j in range(n == 0, 8):
            remote(
                sdir.at[k, j], xbuf.at[quarter, n * 8 + j], s_sem.at[0], sem,
                {
                    "sp_0": (z + ORDER[n]) % NZ,
                    "sp_1": (x + j // 2) % NX,
                    "sp_2": (c + j % 2) % NC,
                },
            ).start()
        return rows

    for quarter in range(NY):
        xbuf[quarter, 0] = direct(quarter, 0, quarter, xs.at[0])[0]
    for n in range(NEAR, NZ):
        direct(NY + n - NEAR, n, far, yrm.at[n])
    loads[7].wait()
    loads[8].wait()

    i0 = lax.broadcasted_iota(jnp.int32, (128, 128), 0)
    i1 = lax.broadcasted_iota(jnp.int32, (128, 128), 1)
    gather = ones_where(i1 == ((i0 >> 2) & 7) * 16 + (i0 >> 5) * 4 + (i0 & 3))
    spread = ones_where(i0 == ((i1 >> 2) & 7) * 16 + (i1 >> 5) * 4 + (i1 & 3))

    def stage_forward(n):
        group = pl.ds(n * 8, 8)

        take(xbuf.at[p, group], xs.at[n])
        remote(xbuf.at[p, group], xbuf.at[p, group], s_sem.at[7], yfm.at[n], at_up).start()
        remote(xbuf.at[p, group], xbuf.at[p, group], s_sem.at[7], yfp.at[n], at_down).start()

    def stage_relay(n):
        group = pl.ds(n * 8, 8)
        front, back = pl.ds(n * 8, 4), pl.ds(n * 8 + 4, 4)
        take(xbuf.at[down, group], yfm.at[n])

        @pl.when(n < NEAR)
        def _():
            remote(xbuf.at[down, front], xbuf.at[down, front], s_sem.at[7], yrm.at[n], at_up).start()

        take(xbuf.at[up, group], yfp.at[n])

        @pl.when(n < NEAR)
        def _():
            remote(xbuf.at[up, back], xbuf.at[up, back], s_sem.at[7], yrp.at[n], at_down).start()


    def stage_hidden(n):
        group = pl.ds(n * 8, 8)
        @pl.when(n == 0)
        def _():
            take(xbuf.at[0, pl.ds(0, 28)], xs.at[0])

        @pl.when(n >= NEAR)
        def _():
            take(xbuf.at[far, group], yrm.at[n])

        @pl.when((n > 0) & (n < NEAR))
        def _():
            take(xbuf.at[far, pl.ds(n * 8, 4)], yrm.at[n])
            take(xbuf.at[far, pl.ds(n * 8 + 4, 4)], yrp.at[n])

        rows = jnp.concatenate([xbuf[k, group].reshape(128, 512) for k in range(NY)], axis=1)
        gate = dot(rows, wg[...])
        hidden = (gate * jax.nn.sigmoid(gate) * dot(rows, wu[...])).astype(bf16)
        hidden = dot(gather, hidden).astype(bf16).reshape(NY, 32, 256)
        hsend[n] = hidden
        for dy in range(1, NY):
            to = (p + dy) % NY
            remote(hsend.at[n, to], hrec.at[n, p], s_sem.at[8], hs.at[n], {"tp": to}).start()
        hrec[n, p] = hsend[n, p]

    def stage_down(n):
        take(hrec.at[n, pl.ds(0, NY - 1)], hs.at[n])
        rows = jnp.concatenate([hrec[n, k] for k in range(NY)], axis=1)
        outs = [
            dot(rows, wd[:, :, 512 * k : 512 * (k + 1)].reshape(1024, 512)).astype(bf16)
            for k in range(4)
        ]
        outs = dot(spread, jnp.concatenate(outs, axis=0)).astype(bf16).reshape(8, 16, 512)
        rsend[pl.ds(n * 8, 8)] = outs
        dz = ring_step(n)
        for j in range(8):
            device = {
                "sp_0": (z + NZ - dz) % NZ,
                "sp_1": (x + NX - j // 2) % NX,
                "sp_2": (c + j % 2) % NC,
            }

            def send(j=j, device=device):
                remote(
                    rsend.at[n * 8 + j], rbuf.at[n * 8 + j], s_sem.at[9], rs.at[n], device
                ).start()

            if j:
                send()
            else:
                pl.when(n > 0)(send)

                @pl.when(n == 0)
                def _():
                    rbuf[0] = outs[0]


    stage_forward(1)
    stage_hidden(0)
    stage_relay(1)
    stage_forward(2)
    stage_hidden(1)

    @pl.loop(3, NZ + 2)
    def _(i):
        @pl.when(i < NZ)
        def _():
            stage_forward(i)

        @pl.when(i < NZ + 1)
        def _():
            stage_relay(i - 1)

        @pl.when((i >= 4) & (i <= NEAR + 1))
        def _():
            stage_hidden(i - 2)

        @pl.when((i >= NEAR + 1) & (i < NZ + 1))
        def _():
            stage_hidden(i - 1)

        @pl.when(i == 3)
        def _():
            for n in range(4):
                take(wd.at[down, pl.ds(32 * (n + 4), 32)], wm.at[n + 4])
                take(wd.at[up, pl.ds(32 * n, 32)], wp.at[n])
            for n in range(8):
                take(wd.at[far, pl.ds(32 * n, 32)], wr.at[n])
            stage_down(0)
            stage_down(1)

        @pl.when((i == NEAR + 1) | (i == NEAR + 2))
        def _():
            stage_down(i - 3)

        @pl.when(i >= NEAR + 2)
        def _():
            stage_down(i - 2)

    picks[...] = jnp.zeros_like(picks)
    own_rows = pl.ds(pl.multiple_of(p * GROUP, GROUP), GROUP)
    base = jnp.concatenate([dcol[0, own_rows, :], dcol[1, own_rows, :]], axis=0)
    base = base - (CAP * p).astype(f32)

    def combine(n, _):
        @pl.when(n == 0)
        def _():
            take(rbuf.at[pl.ds(1, 7)], rs.at[n])

        @pl.when(n > 0)
        def _():
            take(rbuf.at[pl.ds(n * 8, 8)], rs.at[n])

        rows = rbuf[pl.ds(n * 8, 8)].reshape(128, 512)
        for k in range(4):
            pick = jnp.where((i1 + (n * 128 - 4 * k)).astype(f32) == base, 1.0, 0.0).astype(bf16)
            picks[k] = picks[k] + dot(pick, rows)
        return 0

    lax.fori_loop(0, NZ, combine, 0)
    own = mixed[own_rows, :]
    weight = as_column(jnp.concatenate([wsel_ref[0:1, :], wsel_ref[1:2, :]], axis=1), 128)
    for k in range(4):
        cols = slice(512 * k, 512 * (k + 1))
        weighted = weight[:, 0:1] * picks[k]
        routed = weighted[0:64, :] + weighted[64:128, :]
        out_ref[:, cols] = (own[:, cols].astype(f32) + routed).astype(bf16)

    take(wd.at[pl.ds(0, 3)], s_sem.at[1])
    take(cr.at[pl.ds(0, 7)], s_sem.at[2])
    take(crd.at[pl.ds(0, 7)], s_sem.at[10])
    take(zr.at[pl.ds(0, 7)], s_sem.at[3])
    take(zrd.at[pl.ds(0, 7)], s_sem.at[11])
    take(inc.at[pl.ds(0, 7)], s_sem.at[4])
    take(gall.at[pl.ds(0, 3)], s_sem.at[5])
    take(xbuf.at[0, pl.ds(0, 28)], s_sem.at[0])
    take(xbuf.at[0, pl.ds(0, 8 * (NZ - NEAR))], s_sem.at[0])
    take(sbuf.at[pl.ds(0, 56)], s_sem.at[6])
    for k in range(2):
        take(xbuf.at[k, pl.ds(0, 8 * (NZ - 1))], s_sem.at[7])
    take(xbuf.at[2, pl.ds(0, 8 * (NEAR - 1))], s_sem.at[7])
    take(hrec.at[pl.ds(0, 6)], s_sem.at[8])
    take(rbuf.at[pl.ds(0, 63)], s_sem.at[9])


def per_device(
    stream, query, forget_gate_logits, value_input_rows, output_gate_logits, forget_floor_margin,
    additional_fading_speed, head_norm_gain, output_head_weight, feedforward_norm_gain,
    selected_expert_index, selected_expert_weight, expert_gate_weight, expert_up_weight,
    expert_down_weight,
):
    vmem = pl.BlockSpec(memory_space=pltpu.VMEM)
    hbm = pl.BlockSpec(memory_space=pl.ANY)
    dma = pltpu.SemaphoreType.DMA
    V = pltpu.VMEM
    return pl.pallas_call(
        kernel,
        name="layer",
        out_shape=jax.ShapeDtypeStruct((GROUP, 2048), bf16),
        in_specs=[vmem] * 6 + [hbm] * 9,
        out_specs=vmem,
        scratch_shapes=[
            V((ROWS, 256), bf16), V((ROWS, 256), bf16), V((ROWS, 256), bf16), V((ROWS, 256), bf16),
            V((ROWS, 2048), bf16), V((4, 256, 2048), bf16), V((2048, 256), bf16),
            V((2048, 256), bf16), V((4, 256, 2048), bf16),
            V((2, ROWS, 128), f32), V((ROWS, 256), f32), V((8, 32, 128), f32), V((8, 1, 128), f32),
            V((8, 32, 128), f32), V((8, 1, 128), f32), V((8, 32, 128), f32), V((8, 1, 128), f32),
            V((32, 128), f32), V((1, 128), f32), V((8, 32, 128), f32), V((8, 1, 128), f32),
            V((8, 32, 128), f32), V((8, 32, 128), f32), V((2, ROWS), f32), V((2, ROWS, 128), f32),
            V((4, ROWS, 256), bf16), V((ROWS, 2048), f32), V((ROWS, 2048), bf16),
            V((4, ROWS, 512), bf16), V((64, 16, 512), bf16), V((4, 64, 16, 512), bf16),
            V((8, 4, 32, 256), bf16), V((8, 4, 32, 256), bf16), V((64, 16, 512), bf16),
            V((64, 16, 512), bf16), V((4, 128, 512), f32), V((8, 8, 16, 512), bf16),
            dma((9,)), dma((12,)), dma((5,)), dma((3,)), dma((8,)), dma((8,)),
            dma((8,)), dma((8,)), dma((8,)), dma((8,)), dma((8,)), dma((8,)), dma((8,)), dma((8,)),
        ],
        compiler_params=pltpu.CompilerParams(
            collective_id=0, has_side_effects=True, vmem_limit_bytes=60 * 1024 * 1024
        ),
    )(
        selected_expert_index.T, selected_expert_weight.T, forget_floor_margin,
        additional_fading_speed.T, head_norm_gain.reshape(1, 128),
        feedforward_norm_gain.reshape(1, 2048), query, forget_gate_logits, value_input_rows,
        output_gate_logits, stream, output_head_weight.reshape(4, 256, 2048), expert_gate_weight[0],
        expert_up_weight[0], expert_down_weight[0],
    )


def solution(mesh):
    finer = Mesh(mesh.devices.reshape(NZ, NX, NC, mesh.shape["tp"]), SP_TP)
    in_specs = (
        P(SP, None), P(SP, "tp"), P(SP, "tp"), P(SP, "tp"), P(SP, "tp"), P("tp", None),
        P(SP, "tp"), P(), P(), P(), P(SP, None), P(SP_TP, None), P(SP, None, "tp"),
        P(SP, None, "tp"), P(SP, "tp", None),
    )
    return jax.shard_map(
        per_device, mesh=finer, in_specs=in_specs, out_specs=P(SP_TP, None), check_vma=False
    )
```

```python
import functools

import jax
import jax.numpy as jnp
from jax import lax
from jax.experimental import pallas as pl
from jax.experimental.pallas import tpu as pltpu
from jax.sharding import Mesh
from jax.sharding import PartitionSpec as P

SP = ("sp_0", "sp_1", "sp_2")
SP_TP = ("sp_0", "sp_1", "sp_2", "tp")
EPS = 1e-06
f32 = jnp.float32
bf16 = jnp.bfloat16
NZ, NX, NC, NY = 8, 4, 2, 4
ROWS = 256
GROUP = 64
CAP = 4
NT = (((1,), (1,)), ((), ()))


def dot(a, b):
    return jnp.dot(a, b, preferred_element_type=f32)


def dot_nt(a, b):
    return lax.dot_general(a, b, NT, preferred_element_type=f32)


def split2(x):
    high = x.astype(bf16)
    return high, (x - high.astype(f32)).astype(bf16)


def split3(x):
    high = x.astype(bf16)
    rest = x - high.astype(f32)
    mid = rest.astype(bf16)
    return high, mid, (rest - mid.astype(f32)).astype(bf16)


def product_nt(a, b):
    ah, al = split2(a)
    bh, bl = split2(b)
    return dot_nt(jnp.concatenate([ah, ah, al], axis=1), jnp.concatenate([bh, bl, bh], axis=1))


ORDER = (0, 4, 3, 5, 6, 2, 7, 1)
NEAR = 4
PACKED = sum(dz << (3 * n) for n, dz in enumerate(ORDER))


def ring_step(n):
    return (PACKED >> (3 * n)) & 7


def remote(src, dst, send_sem, recv_sem, device):
    return pltpu.make_async_remote_copy(
        src_ref=src,
        dst_ref=dst,
        send_sem=send_sem,
        recv_sem=recv_sem,
        device_id=device,
        device_id_type=pl.DeviceIdType.MESH,
    )


def take(ref, sem):
    pltpu.make_async_copy(ref, ref, sem).wait()


def kernel(
    idx_ref, wsel_ref, mar_ref, fade_ref, hg_ref, fg_ref,
    q_hbm, f_hbm, v_hbm, og_hbm, stream_hbm, wh_hbm, wg_hbm, wu_hbm, wd_hbm,
    out_ref,
    qb, fb, vb, ob, stream, wh, wg, wu, wd,
    rec, qend, cs, csd, cr, crd, px, pxd, us, usd, zr, zrd, isend, inc, dest, dcol,
    gall, acc, mixed, normed, sbuf, xbuf, hsend, hrec, rsend, rbuf, picks, sdir,
    load_sem, s_sem, c_sem, gm, gp, gr, wm, wp, wr, xs, yfm, yfp, yrm, yrp, hs, rs,
):
    z, x, c, p = [lax.axis_index(name) for name in SP_TP]
    up, down, far = (p + 1) % NY, (p + NY - 1) % NY, (p + 2) % NY
    at_up, at_down = {"tp": up}, {"tp": down}

    loads = [
        pltpu.make_async_copy(src, dst, load_sem.at[k])
        for k, (src, dst) in enumerate(
            [
                (f_hbm, fb), (q_hbm, qb), (v_hbm, vb), (wd_hbm, wd.at[p]), (og_hbm, ob),
                (wh_hbm, wh), (stream_hbm, stream), (wg_hbm, wg), (wu_hbm, wu),
            ]
        )
    ]
    for load in loads:
        load.start()

    barrier = pltpu.get_barrier_semaphore()

    def greet(dz, first):
        for k in range(first, NX * NC):
            pl.semaphore_signal(
                barrier,
                inc=1,
                device_id={
                    "sp_0": (z + dz) % NZ, "sp_1": (x + k // 2) % NX, "sp_2": (c + k % 2) % NC,
                },
                device_id_type=pl.DeviceIdType.MESH,
            )

    for peer in (up, down, far):
        pl.semaphore_signal(
            barrier, inc=1, device_id={"tp": peer}, device_id_type=pl.DeviceIdType.MESH
        )
    @pl.loop(1, NZ)
    def _(dz):
        greet(dz, 0)

    greet(0, 1)

    def as_column(line, width):
        return jnp.transpose(jnp.broadcast_to(line, (width, line.shape[1])), (1, 0))

    row = lax.broadcasted_iota(jnp.int32, (ROWS, ROWS), 0)
    col = lax.broadcasted_iota(jnp.int32, (ROWS, ROWS), 1)

    def ones_where(condition):
        return jnp.where(condition, 1.0, 0.0).astype(bf16)

    def level_sum(shift):
        odd = ((row >> shift) & 1) == 1
        same = (row >> shift) == (col >> shift)
        return ones_where(same & ((odd & (col <= row)) | (jnp.logical_not(odd) & (col > row))))

    def inside(h):
        lanes = slice(128 * h, 128 * (h + 1))
        qh, kh = queries[:, lanes], keys[:, lanes]
        exponent = sums_of[3][:, lanes]
        odd = ((row[:, 0:128] >> 3) & 1) == 1
        exponent = jnp.where(odd, exponent, -exponent)
        scores = product_nt(qh * jnp.exp(exponent), kh * jnp.exp(-exponent))
        scores = jnp.where(((row >> 4) == (col >> 4)) & (col <= row), scores, 0.0)
        for shift in (4, 5, 6, 7):
            weight = jnp.exp(sums_of[shift][:, lanes])
            odd = ((row[:, 0:128] >> shift) & 1) == 1
            part = product_nt(jnp.where(odd, qh * weight, 0.0), jnp.where(odd, 0.0, kh * weight))
            scores = scores + jnp.where((row >> (shift + 1)) == (col >> (shift + 1)), part, 0.0)
        sh, sl = split2(scores)
        vh = vb[:, lanes]
        rec[h] = dot(sh, vh) + dot(sl, vh)

    loads[0].wait()
    margin = jnp.concatenate([mar_ref[0:1, :], mar_ref[1:2, :]], axis=1)
    keys = margin * jax.nn.sigmoid(-fb[...].astype(f32))
    fades = jnp.concatenate([as_column(fade_ref[h : h + 1, :], 128) for h in range(2)], axis=1)
    log_decay = jnp.log1p(-keys) + fades
    parts = jnp.concatenate(split3(log_decay), axis=1)

    def sums(matrix):
        three = dot(matrix, parts)
        return three[:, 0:256] + (three[:, 256:512] + three[:, 512:768])

    loads[1].wait()
    loads[2].wait()
    queries = qb[...].astype(f32)
    to_start = sums(ones_where(col <= row))
    to_end = sums(ones_where(col > row))
    qend[...] = queries * jnp.exp(to_start)
    kend = keys * jnp.exp(to_end)
    total = jnp.exp(to_start[ROWS - 1 : ROWS, :])
    vt = jnp.transpose(vb[...].astype(f32), (1, 0)).astype(bf16)
    for h in range(2):
        lanes = slice(128 * h, 128 * (h + 1))
        kh, kl = split2(kend[:, lanes])
        both = dot(vt[lanes, :], jnp.concatenate([kh, kl], axis=1))
        both = both[:, 0:128] + both[:, 128:256]
        for k in range(NX):
            cs[k * NC + h] = both[32 * k : 32 * (k + 1), :]
            csd[k * NC + h] = total[:, lanes]
    sums_of = {shift: sums(level_sum(shift)) for shift in (3, 4, 5, 6, 7)}
    inside(0)
    inside(1)

    chosen = [idx_ref[k : k + 1, :].astype(f32) for k in range(2)]
    columns = [as_column(e, ROWS) for e in chosen]
    block = (row >> 6) == (col >> 6)
    before = block & (row < col)

    def count(condition):
        return jnp.sum(jnp.where(condition, 1.0, 0.0), axis=0, keepdims=True)

    ranks = [
        count(before & (columns[0] == chosen[0])),
        count(block & (columns[0] == chosen[1])) + count(before & (columns[1] == chosen[1])),
    ]
    first_slot = CAP * (lax.broadcasted_iota(jnp.int32, (1, ROWS), 1) >> 6)
    for k in range(2):
        expert = idx_ref[k : k + 1, :]
        dz = ((expert >> 3) + NZ - z) & 7
        group = jnp.zeros_like(dz)
        for n, offset in enumerate(ORDER):
            group = jnp.where(dz == offset, n, group)
        j = (((expert >> 1) + NX - x) & 3) * 2 + ((expert + c) & 1)
        place = ((group * 8 + j) * 16 + first_slot).astype(f32) + ranks[k]
        dest[k : k + 1, :] = place
        dcol[k] = as_column(place, 128)

    pl.semaphore_wait(barrier, NZ * NX * NC - 1 + 3)

    def down_weights(n):
        rows, other = pl.ds(32 * n, 32), pl.ds(32 * (7 - n), 32)
        remote(wd.at[p, rows], wd.at[p, rows], s_sem.at[1], wm.at[n], at_up).start()
        remote(wd.at[p, other], wd.at[p, other], s_sem.at[1], wp.at[7 - n], at_down).start()

    for dx in (2, 1, 3, 0):
        to = (x + dx) % NX
        for dc in range(NC):
            if dx or dc:
                head = (c + dc) % NC
                device = {"sp_1": to, "sp_2": head}
                remote(
                    cs.at[to * NC + head], cr.at[x * NC + c], s_sem.at[2], c_sem.at[1], device
                ).start()
                remote(
                    csd.at[to * NC + head], crd.at[x * NC + c], s_sem.at[10], c_sem.at[0], device
                ).start()
    loads[3].wait()
    for n in range(4):
        down_weights(n)
    cr[x * NC + c] = cs[x * NC + c]
    crd[x * NC + c] = csd[x * NC + c]
    take(cr.at[pl.ds(0, NX * NC - 1)], c_sem.at[1])
    take(crd.at[pl.ds(0, NX * NC - 1)], c_sem.at[0])
    state, decay = jnp.zeros((32, 128), f32), jnp.ones((1, 128), f32)
    for k in range(NX * NC):
        px[k] = state
        pxd[k] = decay
        state = crd[k] * state + cr[k]
        decay = crd[k] * decay
    us[...] = state
    usd[...] = decay
    for dz in (4, 3, 5, 2, 6, 1, 7):
        device = {"sp_0": (z + dz) % NZ}
        remote(us, zr.at[z], s_sem.at[3], c_sem.at[2], device).start()
        remote(usd, zrd.at[z], s_sem.at[11], c_sem.at[4], device).start()
    zr[z] = us[...]
    zrd[z] = usd[...]
    take(zr.at[pl.ds(0, NZ - 1)], c_sem.at[2])
    take(zrd.at[pl.ds(0, NZ - 1)], c_sem.at[4])
    state = jnp.zeros((32, 128), f32)
    for k in range(NZ):
        counts = (k < z).astype(f32)
        state = (1.0 - counts) * state + counts * (zrd[k] * state + zr[k])
    for k in range(NX * NC):
        isend[k] = pxd[k] * state + px[k]
    for dx in (2, 1, 3, 0):
        to = (x + dx) % NX
        for dc in range(NC):
            if dx or dc:
                core = (c + dc) % NC
                remote(
                    isend.at[to * NC + core], inc.at[c * NX + x], s_sem.at[4], c_sem.at[3],
                    {"sp_1": to, "sp_2": core},
                ).start()
    inc[c * NX + x] = isend[x * NC + c]
    down_weights(4)
    take(inc.at[pl.ds(0, NX * NC - 1)], c_sem.at[3])

    loads[4].wait()
    for h in range(2):
        lanes = slice(128 * h, 128 * (h + 1))
        before = inc[NX * h : NX * (h + 1)].reshape(128, 128)
        recur = rec[h] + product_nt(qend[:, lanes], before)
        scale = lax.rsqrt(jnp.mean(recur * recur, axis=-1, keepdims=True) + EPS)
        gate_in = ob[:, lanes].astype(f32)
        gated = recur * scale * hg_ref[...] * (gate_in * jax.nn.sigmoid(gate_in))
        gall[p, :, lanes] = gated.astype(bf16)

    for half in range(2):
        rows = pl.ds(128 * half, 128)
        other = pl.ds(128 * (1 - half), 128)
        remote(gall.at[p, rows], gall.at[p, rows], s_sem.at[5], gm.at[half], at_up).start()
        remote(gall.at[p, other], gall.at[p, other], s_sem.at[5], gp.at[1 - half], at_down).start()
    low, high = pl.ds(0, 128), pl.ds(128, 128)
    loads[5].wait()

    def project(source, fresh):
        lhs = gall[source]
        for k in range(4):
            cols = slice(512 * k, 512 * (k + 1))
            part = dot(lhs, wh[source, :, cols])
            if fresh:
                acc[:, cols] = part
            else:
                acc[:, cols] = acc[:, cols] + part

    project(p, True)
    take(gall.at[down, low], gm.at[0])
    remote(gall.at[down, low], gall.at[down, low], s_sem.at[5], gr.at[0], at_up).start()
    take(gall.at[up, high], gp.at[1])
    remote(gall.at[up, high], gall.at[up, high], s_sem.at[5], gr.at[1], at_down).start()
    down_weights(5)
    down_weights(6)
    for n in range(4):
        rows, other = pl.ds(32 * n, 32), pl.ds(32 * (7 - n), 32)
        take(wd.at[down, rows], wm.at[n])
        remote(wd.at[down, rows], wd.at[down, rows], s_sem.at[1], wr.at[n], at_up).start()
        take(wd.at[up, other], wp.at[7 - n])
        remote(wd.at[up, other], wd.at[up, other], s_sem.at[1], wr.at[7 - n], at_down).start()
    down_weights(7)
    take(gall.at[down, high], gm.at[1])
    project(down, False)
    take(gall.at[up, low], gp.at[0])
    project(up, False)
    take(gall.at[far, low], gr.at[0])
    take(gall.at[far, high], gr.at[1])
    project(far, False)

    loads[6].wait()
    gain = fg_ref[...]

    def norm_rows(k, _):
        rows = pl.ds(pl.multiple_of(k * 32, 32), 32)
        wide = (stream[rows, :].astype(f32) + acc[rows, :]).astype(bf16)
        mixed[rows, :] = wide
        wide = wide.astype(f32)
        scale = lax.rsqrt(jnp.mean(wide * wide, axis=-1, keepdims=True) + EPS)
        done = (wide * scale * gain).astype(bf16)
        for quarter in range(4):
            normed[quarter, rows, :] = done[:, 512 * quarter : 512 * (quarter + 1)]
        return 0

    lax.fori_loop(0, ROWS // 32, norm_rows, 0)

    dest0, dest1 = dest[0:1, :], dest[1:2, :]
    slot = lax.broadcasted_iota(jnp.int32, (128, ROWS), 0)

    def slots_of(n, quarter):
        ids = (slot + n * 128).astype(f32)
        pick = jnp.where((ids == dest0) | (ids == dest1), 1.0, 0.0).astype(bf16)
        return dot(pick, normed[quarter]).astype(bf16).reshape(8, 16, 512)

    def dispatch(n, _):
        sbuf[pl.ds(n * 8, 8)] = slots_of(n, p)
        dz = ring_step(n)
        for j in range(8):
            remote(
                sbuf.at[n * 8 + j], xbuf.at[p, n * 8 + j], s_sem.at[6], xs.at[n],
                {"sp_0": (z + dz) % NZ, "sp_1": (x + j // 2) % NX, "sp_2": (c + j % 2) % NC},
            ).start()
        return 0

    lax.fori_loop(1, NZ, dispatch, 0)
    def direct(k, n, quarter, sem):
        rows = slots_of(n, quarter)
        sdir[k] = rows
        for j in range(n == 0, 8):
            remote(
                sdir.at[k, j], xbuf.at[quarter, n * 8 + j], s_sem.at[0], sem,
                {
                    "sp_0": (z + ORDER[n]) % NZ,
                    "sp_1": (x + j // 2) % NX,
                    "sp_2": (c + j % 2) % NC,
                },
            ).start()
        return rows

    for quarter in range(NY):
        xbuf[quarter, 0] = direct(quarter, 0, quarter, xs.at[0])[0]
    for n in range(NEAR, NZ):
        direct(NY + n - NEAR, n, far, yrm.at[n])
    loads[7].wait()
    loads[8].wait()

    i0 = lax.broadcasted_iota(jnp.int32, (128, 128), 0)
    i1 = lax.broadcasted_iota(jnp.int32, (128, 128), 1)
    gather = ones_where(i1 == ((i0 >> 2) & 7) * 16 + (i0 >> 5) * 4 + (i0 & 3))
    spread = ones_where(i0 == ((i1 >> 2) & 7) * 16 + (i1 >> 5) * 4 + (i1 & 3))

    def stage_forward(n):
        group = pl.ds(n * 8, 8)

        take(xbuf.at[p, group], xs.at[n])
        remote(xbuf.at[p, group], xbuf.at[p, group], s_sem.at[7], yfm.at[n], at_up).start()
        remote(xbuf.at[p, group], xbuf.at[p, group], s_sem.at[7], yfp.at[n], at_down).start()

    def stage_relay(n):
        group = pl.ds(n * 8, 8)
        front, back = pl.ds(n * 8, 4), pl.ds(n * 8 + 4, 4)
        take(xbuf.at[down, group], yfm.at[n])

        @pl.when(n < NEAR)
        def _():
            remote(xbuf.at[down, front], xbuf.at[down, front], s_sem.at[7], yrm.at[n], at_up).start()

        take(xbuf.at[up, group], yfp.at[n])

        @pl.when(n < NEAR)
        def _():
            remote(xbuf.at[up, back], xbuf.at[up, back], s_sem.at[7], yrp.at[n], at_down).start()


    def stage_hidden(n):
        group = pl.ds(n * 8, 8)
        @pl.when(n == 0)
        def _():
            take(xbuf.at[0, pl.ds(0, 28)], xs.at[0])

        @pl.when(n >= NEAR)
        def _():
            take(xbuf.at[far, group], yrm.at[n])

        @pl.when((n > 0) & (n < NEAR))
        def _():
            take(xbuf.at[far, pl.ds(n * 8, 4)], yrm.at[n])
            take(xbuf.at[far, pl.ds(n * 8 + 4, 4)], yrp.at[n])

        rows = jnp.concatenate([xbuf[k, group].reshape(128, 512) for k in range(NY)], axis=1)
        gate = dot(rows, wg[...])
        hidden = (gate * jax.nn.sigmoid(gate) * dot(rows, wu[...])).astype(bf16)
        hidden = dot(gather, hidden).astype(bf16).reshape(NY, 32, 256)
        hsend[n] = hidden
        for dy in range(1, NY):
            to = (p + dy) % NY
            remote(hsend.at[n, to], hrec.at[n, p], s_sem.at[8], hs.at[n], {"tp": to}).start()
        hrec[n, p] = hsend[n, p]

    def stage_down(n):
        take(hrec.at[n, pl.ds(0, NY - 1)], hs.at[n])
        rows = jnp.concatenate([hrec[n, k] for k in range(NY)], axis=1)
        outs = [
            dot(rows, wd[:, :, 512 * k : 512 * (k + 1)].reshape(1024, 512)).astype(bf16)
            for k in range(4)
        ]
        outs = dot(spread, jnp.concatenate(outs, axis=0)).astype(bf16).reshape(8, 16, 512)
        rsend[pl.ds(n * 8, 8)] = outs
        dz = ring_step(n)
        for j in range(8):
            device = {
                "sp_0": (z + NZ - dz) % NZ,
                "sp_1": (x + NX - j // 2) % NX,
                "sp_2": (c + j % 2) % NC,
            }

            def send(j=j, device=device):
                remote(
                    rsend.at[n * 8 + j], rbuf.at[n * 8 + j], s_sem.at[9], rs.at[n], device
                ).start()

            if j:
                send()
            else:
                pl.when(n > 0)(send)

                @pl.when(n == 0)
                def _():
                    rbuf[0] = outs[0]


    stage_forward(1)
    stage_hidden(0)
    stage_relay(1)
    stage_forward(2)
    stage_hidden(1)

    @pl.loop(3, NZ + 2)
    def _(i):
        @pl.when(i < NZ)
        def _():
            stage_forward(i)

        @pl.when(i < NZ + 1)
        def _():
            stage_relay(i - 1)

        @pl.when((i >= 4) & (i <= NEAR + 1))
        def _():
            stage_hidden(i - 2)

        @pl.when((i >= NEAR + 1) & (i < NZ + 1))
        def _():
            stage_hidden(i - 1)

        @pl.when(i == 3)
        def _():
            for n in range(4):
                take(wd.at[down, pl.ds(32 * (n + 4), 32)], wm.at[n + 4])
                take(wd.at[up, pl.ds(32 * n, 32)], wp.at[n])
            for n in range(8):
                take(wd.at[far, pl.ds(32 * n, 32)], wr.at[n])
            stage_down(0)
            stage_down(1)

        @pl.when((i == NEAR + 1) | (i == NEAR + 2))
        def _():
            stage_down(i - 3)

        @pl.when(i >= NEAR + 2)
        def _():
            stage_down(i - 2)

    picks[...] = jnp.zeros_like(picks)
    own_rows = pl.ds(pl.multiple_of(p * GROUP, GROUP), GROUP)
    base = jnp.concatenate([dcol[0, own_rows, :], dcol[1, own_rows, :]], axis=0)
    base = base - (CAP * p).astype(f32)

    def combine(n, _):
        @pl.when(n == 0)
        def _():
            take(rbuf.at[pl.ds(1, 7)], rs.at[n])

        @pl.when(n > 0)
        def _():
            take(rbuf.at[pl.ds(n * 8, 8)], rs.at[n])

        rows = rbuf[pl.ds(n * 8, 8)].reshape(128, 512)
        for k in range(4):
            pick = jnp.where((i1 + (n * 128 - 4 * k)).astype(f32) == base, 1.0, 0.0).astype(bf16)
            picks[k] = picks[k] + dot(pick, rows)
        return 0

    lax.fori_loop(0, NZ, combine, 0)
    own = mixed[own_rows, :]
    weight = as_column(jnp.concatenate([wsel_ref[0:1, :], wsel_ref[1:2, :]], axis=1), 128)
    for k in range(4):
        cols = slice(512 * k, 512 * (k + 1))
        weighted = weight[:, 0:1] * picks[k]
        routed = weighted[0:64, :] + weighted[64:128, :]
        out_ref[:, cols] = (own[:, cols].astype(f32) + routed).astype(bf16)

    take(wd.at[pl.ds(0, 3)], s_sem.at[1])
    take(cr.at[pl.ds(0, 7)], s_sem.at[2])
    take(crd.at[pl.ds(0, 7)], s_sem.at[10])
    take(zr.at[pl.ds(0, 7)], s_sem.at[3])
    take(zrd.at[pl.ds(0, 7)], s_sem.at[11])
    take(inc.at[pl.ds(0, 7)], s_sem.at[4])
    take(gall.at[pl.ds(0, 3)], s_sem.at[5])
    take(xbuf.at[0, pl.ds(0, 28)], s_sem.at[0])
    take(xbuf.at[0, pl.ds(0, 8 * (NZ - NEAR))], s_sem.at[0])
    take(sbuf.at[pl.ds(0, 56)], s_sem.at[6])
    for k in range(2):
        take(xbuf.at[k, pl.ds(0, 8 * (NZ - 1))], s_sem.at[7])
    take(xbuf.at[2, pl.ds(0, 8 * (NEAR - 1))], s_sem.at[7])
    take(hrec.at[pl.ds(0, 6)], s_sem.at[8])
    take(rbuf.at[pl.ds(0, 63)], s_sem.at[9])


def per_device(
    stream, query, forget_gate_logits, value_input_rows, output_gate_logits, forget_floor_margin,
    additional_fading_speed, head_norm_gain, output_head_weight, feedforward_norm_gain,
    selected_expert_index, selected_expert_weight, expert_gate_weight, expert_up_weight,
    expert_down_weight,
):
    vmem = pl.BlockSpec(memory_space=pltpu.VMEM)
    hbm = pl.BlockSpec(memory_space=pl.ANY)
    dma = pltpu.SemaphoreType.DMA
    V = pltpu.VMEM
    return pl.pallas_call(
        kernel,
        name="layer",
        out_shape=jax.ShapeDtypeStruct((GROUP, 2048), bf16),
        in_specs=[vmem] * 6 + [hbm] * 9,
        out_specs=vmem,
        scratch_shapes=[
            V((ROWS, 256), bf16), V((ROWS, 256), bf16), V((ROWS, 256), bf16), V((ROWS, 256), bf16),
            V((ROWS, 2048), bf16), V((4, 256, 2048), bf16), V((2048, 256), bf16),
            V((2048, 256), bf16), V((4, 256, 2048), bf16),
            V((2, ROWS, 128), f32), V((ROWS, 256), f32), V((8, 32, 128), f32), V((8, 1, 128), f32),
            V((8, 32, 128), f32), V((8, 1, 128), f32), V((8, 32, 128), f32), V((8, 1, 128), f32),
            V((32, 128), f32), V((1, 128), f32), V((8, 32, 128), f32), V((8, 1, 128), f32),
            V((8, 32, 128), f32), V((8, 32, 128), f32), V((2, ROWS), f32), V((2, ROWS, 128), f32),
            V((4, ROWS, 256), bf16), V((ROWS, 2048), f32), V((ROWS, 2048), bf16),
            V((4, ROWS, 512), bf16), V((64, 16, 512), bf16), V((4, 64, 16, 512), bf16),
            V((8, 4, 32, 256), bf16), V((8, 4, 32, 256), bf16), V((64, 16, 512), bf16),
            V((64, 16, 512), bf16), V((4, 128, 512), f32), V((8, 8, 16, 512), bf16),
            dma((9,)), dma((12,)), dma((5,)), dma((2,)), dma((2,)), dma((2,)), dma((8,)), dma((8,)),
            dma((8,)), dma((8,)), dma((8,)), dma((8,)), dma((8,)), dma((8,)), dma((8,)), dma((8,)),
        ],
        compiler_params=pltpu.CompilerParams(
            collective_id=0, has_side_effects=True, vmem_limit_bytes=60 * 1024 * 1024
        ),
    )(
        selected_expert_index.T, selected_expert_weight.T, forget_floor_margin,
        additional_fading_speed.T, head_norm_gain.reshape(1, 128),
        feedforward_norm_gain.reshape(1, 2048), query, forget_gate_logits, value_input_rows,
        output_gate_logits, stream, output_head_weight.reshape(4, 256, 2048), expert_gate_weight[0],
        expert_up_weight[0], expert_down_weight[0],
    )


def solution(mesh):
    finer = Mesh(mesh.devices.reshape(NZ, NX, NC, mesh.shape["tp"]), SP_TP)
    in_specs = (
        P(SP, None), P(SP, "tp"), P(SP, "tp"), P(SP, "tp"), P(SP, "tp"), P("tp", None),
        P(SP, "tp"), P(), P(), P(), P(SP, None), P(SP_TP, None), P(SP, None, "tp"),
        P(SP, None, "tp"), P(SP, "tp", None),
    )
    return jax.shard_map(
        per_device, mesh=finer, in_specs=in_specs, out_specs=P(SP_TP, None), check_vma=False
    )
```

```python
import functools

import jax
import jax.numpy as jnp
from jax import lax
from jax.experimental import pallas as pl
from jax.experimental.pallas import tpu as pltpu
from jax.sharding import Mesh
from jax.sharding import PartitionSpec as P

SP = ("sp_0", "sp_1", "sp_2")
SP_TP = ("sp_0", "sp_1", "sp_2", "tp")
EPS = 1e-06
f32 = jnp.float32
bf16 = jnp.bfloat16
NZ, NX, NC, NY = 8, 4, 2, 4
ROWS = 256
GROUP = 64
CAP = 4
NT = (((1,), (1,)), ((), ()))


def dot(a, b):
    return jnp.dot(a, b, preferred_element_type=f32)


def dot_nt(a, b):
    return lax.dot_general(a, b, NT, preferred_element_type=f32)


def split2(x):
    high = x.astype(bf16)
    return high, (x - high.astype(f32)).astype(bf16)


def split3(x):
    high = x.astype(bf16)
    rest = x - high.astype(f32)
    mid = rest.astype(bf16)
    return high, mid, (rest - mid.astype(f32)).astype(bf16)


def product_nt(a, b):
    ah, al = split2(a)
    bh, bl = split2(b)
    return dot_nt(jnp.concatenate([ah, ah, al], axis=1), jnp.concatenate([bh, bl, bh], axis=1))


ORDER = (0, 4, 3, 5, 6, 2, 7, 1)
NEAR = 6
PACKED = sum(dz << (3 * n) for n, dz in enumerate(ORDER))


def ring_step(n):
    return (PACKED >> (3 * n)) & 7


def remote(src, dst, send_sem, recv_sem, device):
    return pltpu.make_async_remote_copy(
        src_ref=src,
        dst_ref=dst,
        send_sem=send_sem,
        recv_sem=recv_sem,
        device_id=device,
        device_id_type=pl.DeviceIdType.MESH,
    )


def take(ref, sem):
    pltpu.make_async_copy(ref, ref, sem).wait()


def kernel(
    idx_ref, wsel_ref, mar_ref, fade_ref, hg_ref, fg_ref,
    q_hbm, f_hbm, v_hbm, og_hbm, stream_hbm, wh_hbm, wg_hbm, wu_hbm, wd_hbm,
    out_ref,
    qb, fb, vb, ob, stream, wh, wg, wu, wd,
    rec, qend, cs, csd, cr, crd, px, pxd, us, usd, zr, zrd, isend, inc, dest, dcol,
    gall, acc, mixed, normed, sbuf, xbuf, hsend, hrec, rsend, rbuf, picks, sdir,
    load_sem, s_sem, c_sem, gm, gp, gr, wm, wp, wr, xs, yfm, yfp, yrm, yrp, hs, rs,
):
    z, x, c, p = [lax.axis_index(name) for name in SP_TP]
    up, down, far = (p + 1) % NY, (p + NY - 1) % NY, (p + 2) % NY
    at_up, at_down = {"tp": up}, {"tp": down}

    loads = [
        pltpu.make_async_copy(src, dst, load_sem.at[k])
        for k, (src, dst) in enumerate(
            [
                (f_hbm, fb), (q_hbm, qb), (v_hbm, vb), (wd_hbm, wd.at[p]), (og_hbm, ob),
                (wh_hbm, wh), (stream_hbm, stream), (wg_hbm, wg), (wu_hbm, wu),
            ]
        )
    ]
    for load in loads:
        load.start()

    barrier = pltpu.get_barrier_semaphore()

    def greet(dz, first):
        for k in range(first, NX * NC):
            pl.semaphore_signal(
                barrier,
                inc=1,
                device_id={
                    "sp_0": (z + dz) % NZ, "sp_1": (x + k // 2) % NX, "sp_2": (c + k % 2) % NC,
                },
                device_id_type=pl.DeviceIdType.MESH,
            )

    for peer in (up, down, far):
        pl.semaphore_signal(
            barrier, inc=1, device_id={"tp": peer}, device_id_type=pl.DeviceIdType.MESH
        )
    @pl.loop(1, NZ)
    def _(dz):
        greet(dz, 0)

    greet(0, 1)

    def as_column(line, width):
        return jnp.transpose(jnp.broadcast_to(line, (width, line.shape[1])), (1, 0))

    row = lax.broadcasted_iota(jnp.int32, (ROWS, ROWS), 0)
    col = lax.broadcasted_iota(jnp.int32, (ROWS, ROWS), 1)

    def ones_where(condition):
        return jnp.where(condition, 1.0, 0.0).astype(bf16)

    def level_sum(shift):
        odd = ((row >> shift) & 1) == 1
        same = (row >> shift) == (col >> shift)
        return ones_where(same & ((odd & (col <= row)) | (jnp.logical_not(odd) & (col > row))))

    def inside(h):
        lanes = slice(128 * h, 128 * (h + 1))
        qh, kh = queries[:, lanes], keys[:, lanes]
        exponent = sums_of[3][:, lanes]
        odd = ((row[:, 0:128] >> 3) & 1) == 1
        exponent = jnp.where(odd, exponent, -exponent)
        scores = product_nt(qh * jnp.exp(exponent), kh * jnp.exp(-exponent))
        scores = jnp.where(((row >> 4) == (col >> 4)) & (col <= row), scores, 0.0)
        for shift in (4, 5, 6, 7):
            weight = jnp.exp(sums_of[shift][:, lanes])
            odd = ((row[:, 0:128] >> shift) & 1) == 1
            part = product_nt(jnp.where(odd, qh * weight, 0.0), jnp.where(odd, 0.0, kh * weight))
            scores = scores + jnp.where((row >> (shift + 1)) == (col >> (shift + 1)), part, 0.0)
        sh, sl = split2(scores)
        vh = vb[:, lanes]
        rec[h] = dot(sh, vh) + dot(sl, vh)

    loads[0].wait()
    margin = jnp.concatenate([mar_ref[0:1, :], mar_ref[1:2, :]], axis=1)
    keys = margin * jax.nn.sigmoid(-fb[...].astype(f32))
    fades = jnp.concatenate([as_column(fade_ref[h : h + 1, :], 128) for h in range(2)], axis=1)
    log_decay = jnp.log1p(-keys) + fades
    parts = jnp.concatenate(split3(log_decay), axis=1)

    def sums(matrix):
        three = dot(matrix, parts)
        return three[:, 0:256] + (three[:, 256:512] + three[:, 512:768])

    loads[1].wait()
    loads[2].wait()
    queries = qb[...].astype(f32)
    to_start = sums(ones_where(col <= row))
    to_end = sums(ones_where(col > row))
    qend[...] = queries * jnp.exp(to_start)
    kend = keys * jnp.exp(to_end)
    total = jnp.exp(to_start[ROWS - 1 : ROWS, :])
    vt = jnp.transpose(vb[...].astype(f32), (1, 0)).astype(bf16)
    for h in range(2):
        lanes = slice(128 * h, 128 * (h + 1))
        kh, kl = split2(kend[:, lanes])
        both = dot(vt[lanes, :], jnp.concatenate([kh, kl], axis=1))
        both = both[:, 0:128] + both[:, 128:256]
        for k in range(NX):
            cs[k * NC + h] = both[32 * k : 32 * (k + 1), :]
            csd[k * NC + h] = total[:, lanes]
    sums_of = {shift: sums(level_sum(shift)) for shift in (3, 4, 5, 6, 7)}
    inside(0)
    inside(1)

    chosen = [idx_ref[k : k + 1, :].astype(f32) for k in range(2)]
    columns = [as_column(e, ROWS) for e in chosen]
    block = (row >> 6) == (col >> 6)
    before = block & (row < col)

    def count(condition):
        return jnp.sum(jnp.where(condition, 1.0, 0.0), axis=0, keepdims=True)

    ranks = [
        count(before & (columns[0] == chosen[0])),
        count(block & (columns[0] == chosen[1])) + count(before & (columns[1] == chosen[1])),
    ]
    first_slot = CAP * (lax.broadcasted_iota(jnp.int32, (1, ROWS), 1) >> 6)
    for k in range(2):
        expert = idx_ref[k : k + 1, :]
        dz = ((expert >> 3) + NZ - z) & 7
        group = jnp.zeros_like(dz)
        for n, offset in enumerate(ORDER):
            group = jnp.where(dz == offset, n, group)
        j = (((expert >> 1) + NX - x) & 3) * 2 + ((expert + c) & 1)
        place = ((group * 8 + j) * 16 + first_slot).astype(f32) + ranks[k]
        dest[k : k + 1, :] = place
        dcol[k] = as_column(place, 128)

    pl.semaphore_wait(barrier, NZ * NX * NC - 1 + 3)

    def down_weights(n):
        rows, other = pl.ds(32 * n, 32), pl.ds(32 * (7 - n), 32)
        remote(wd.at[p, rows], wd.at[p, rows], s_sem.at[1], wm.at[n], at_up).start()
        remote(wd.at[p, other], wd.at[p, other], s_sem.at[1], wp.at[7 - n], at_down).start()

    for dx in (2, 1, 3, 0):
        to = (x + dx) % NX
        for dc in range(NC):
            if dx or dc:
                head = (c + dc) % NC
                device = {"sp_1": to, "sp_2": head}
                remote(
                    cs.at[to * NC + head], cr.at[x * NC + c], s_sem.at[2], c_sem.at[1], device
                ).start()
                remote(
                    csd.at[to * NC + head], crd.at[x * NC + c], s_sem.at[10], c_sem.at[0], device
                ).start()
    loads[3].wait()
    for n in range(4):
        down_weights(n)
    cr[x * NC + c] = cs[x * NC + c]
    crd[x * NC + c] = csd[x * NC + c]
    take(cr.at[pl.ds(0, NX * NC - 1)], c_sem.at[1])
    take(crd.at[pl.ds(0, NX * NC - 1)], c_sem.at[0])
    state, decay = jnp.zeros((32, 128), f32), jnp.ones((1, 128), f32)
    for k in range(NX * NC):
        px[k] = state
        pxd[k] = decay
        state = crd[k] * state + cr[k]
        decay = crd[k] * decay
    us[...] = state
    usd[...] = decay
    for dz in (4, 3, 5, 2, 6, 1, 7):
        device = {"sp_0": (z + dz) % NZ}
        remote(us, zr.at[z], s_sem.at[3], c_sem.at[2], device).start()
        remote(usd, zrd.at[z], s_sem.at[11], c_sem.at[4], device).start()
    zr[z] = us[...]
    zrd[z] = usd[...]
    take(zr.at[pl.ds(0, NZ - 1)], c_sem.at[2])
    take(zrd.at[pl.ds(0, NZ - 1)], c_sem.at[4])
    state = jnp.zeros((32, 128), f32)
    for k in range(NZ):
        counts = (k < z).astype(f32)
        state = (1.0 - counts) * state + counts * (zrd[k] * state + zr[k])
    for k in range(NX * NC):
        isend[k] = pxd[k] * state + px[k]
    for dx in (2, 1, 3, 0):
        to = (x + dx) % NX
        for dc in range(NC):
            if dx or dc:
                core = (c + dc) % NC
                remote(
                    isend.at[to * NC + core], inc.at[c * NX + x], s_sem.at[4], c_sem.at[3],
                    {"sp_1": to, "sp_2": core},
                ).start()
    inc[c * NX + x] = isend[x * NC + c]
    down_weights(4)
    take(inc.at[pl.ds(0, NX * NC - 1)], c_sem.at[3])

    loads[4].wait()
    for h in range(2):
        lanes = slice(128 * h, 128 * (h + 1))
        before = inc[NX * h : NX * (h + 1)].reshape(128, 128)
        recur = rec[h] + product_nt(qend[:, lanes], before)
        scale = lax.rsqrt(jnp.mean(recur * recur, axis=-1, keepdims=True) + EPS)
        gate_in = ob[:, lanes].astype(f32)
        gated = recur * scale * hg_ref[...] * (gate_in * jax.nn.sigmoid(gate_in))
        gall[p, :, lanes] = gated.astype(bf16)

    for half in range(2):
        rows = pl.ds(128 * half, 128)
        other = pl.ds(128 * (1 - half), 128)
        remote(gall.at[p, rows], gall.at[p, rows], s_sem.at[5], gm.at[half], at_up).start()
        remote(gall.at[p, other], gall.at[p, other], s_sem.at[5], gp.at[1 - half], at_down).start()
    low, high = pl.ds(0, 128), pl.ds(128, 128)
    loads[5].wait()

    def project(source, fresh):
        lhs = gall[source]
        for k in range(4):
            cols = slice(512 * k, 512 * (k + 1))
            part = dot(lhs, wh[source, :, cols])
            if fresh:
                acc[:, cols] = part
            else:
                acc[:, cols] = acc[:, cols] + part

    project(p, True)
    take(gall.at[down, low], gm.at[0])
    remote(gall.at[down, low], gall.at[down, low], s_sem.at[5], gr.at[0], at_up).start()
    take(gall.at[up, high], gp.at[1])
    remote(gall.at[up, high], gall.at[up, high], s_sem.at[5], gr.at[1], at_down).start()
    down_weights(5)
    down_weights(6)
    for n in range(4):
        rows, other = pl.ds(32 * n, 32), pl.ds(32 * (7 - n), 32)
        take(wd.at[down, rows], wm.at[n])
        remote(wd.at[down, rows], wd.at[down, rows], s_sem.at[1], wr.at[n], at_up).start()
        take(wd.at[up, other], wp.at[7 - n])
        remote(wd.at[up, other], wd.at[up, other], s_sem.at[1], wr.at[7 - n], at_down).start()
    down_weights(7)
    take(gall.at[down, high], gm.at[1])
    project(down, False)
    take(gall.at[up, low], gp.at[0])
    project(up, False)
    take(gall.at[far, low], gr.at[0])
    take(gall.at[far, high], gr.at[1])
    project(far, False)

    loads[6].wait()
    gain = fg_ref[...]

    def norm_rows(k, _):
        rows = pl.ds(pl.multiple_of(k * 32, 32), 32)
        wide = (stream[rows, :].astype(f32) + acc[rows, :]).astype(bf16)
        mixed[rows, :] = wide
        wide = wide.astype(f32)
        scale = lax.rsqrt(jnp.mean(wide * wide, axis=-1, keepdims=True) + EPS)
        done = (wide * scale * gain).astype(bf16)
        for quarter in range(4):
            normed[quarter, rows, :] = done[:, 512 * quarter : 512 * (quarter + 1)]
        return 0

    lax.fori_loop(0, ROWS // 32, norm_rows, 0)

    dest0, dest1 = dest[0:1, :], dest[1:2, :]
    slot = lax.broadcasted_iota(jnp.int32, (128, ROWS), 0)

    def slots_of(n, quarter):
        ids = (slot + n * 128).astype(f32)
        pick = jnp.where((ids == dest0) | (ids == dest1), 1.0, 0.0).astype(bf16)
        return dot(pick, normed[quarter]).astype(bf16).reshape(8, 16, 512)

    def dispatch(n, _):
        sbuf[pl.ds(n * 8, 8)] = slots_of(n, p)
        dz = ring_step(n)
        for j in range(8):
            remote(
                sbuf.at[n * 8 + j], xbuf.at[p, n * 8 + j], s_sem.at[6], xs.at[n],
                {"sp_0": (z + dz) % NZ, "sp_1": (x + j // 2) % NX, "sp_2": (c + j % 2) % NC},
            ).start()
        return 0

    lax.fori_loop(1, NZ, dispatch, 0)
    def direct(k, n, quarter, sem):
        rows = slots_of(n, quarter)
        sdir[k] = rows
        for j in range(n == 0, 8):
            remote(
                sdir.at[k, j], xbuf.at[quarter, n * 8 + j], s_sem.at[0], sem,
                {
                    "sp_0": (z + ORDER[n]) % NZ,
                    "sp_1": (x + j // 2) % NX,
                    "sp_2": (c + j % 2) % NC,
                },
            ).start()
        return rows

    for quarter in range(NY):
        xbuf[quarter, 0] = direct(quarter, 0, quarter, xs.at[0])[0]
    for n in range(NEAR, NZ):
        direct(NY + n - NEAR, n, far, yrm.at[n])
    loads[7].wait()
    loads[8].wait()

    i0 = lax.broadcasted_iota(jnp.int32, (128, 128), 0)
    i1 = lax.broadcasted_iota(jnp.int32, (128, 128), 1)
    gather = ones_where(i1 == ((i0 >> 2) & 7) * 16 + (i0 >> 5) * 4 + (i0 & 3))
    spread = ones_where(i0 == ((i1 >> 2) & 7) * 16 + (i1 >> 5) * 4 + (i1 & 3))

    def stage_forward(n):
        group = pl.ds(n * 8, 8)

        take(xbuf.at[p, group], xs.at[n])
        remote(xbuf.at[p, group], xbuf.at[p, group], s_sem.at[7], yfm.at[n], at_up).start()
        remote(xbuf.at[p, group], xbuf.at[p, group], s_sem.at[7], yfp.at[n], at_down).start()

    def stage_relay(n):
        group = pl.ds(n * 8, 8)
        front, back = pl.ds(n * 8, 4), pl.ds(n * 8 + 4, 4)
        take(xbuf.at[down, group], yfm.at[n])

        @pl.when(n < NEAR)
        def _():
            remote(xbuf.at[down, front], xbuf.at[down, front], s_sem.at[7], yrm.at[n], at_up).start()

        take(xbuf.at[up, group], yfp.at[n])

        @pl.when(n < NEAR)
        def _():
            remote(xbuf.at[up, back], xbuf.at[up, back], s_sem.at[7], yrp.at[n], at_down).start()


    def stage_hidden(n):
        group = pl.ds(n * 8, 8)
        @pl.when(n == 0)
        def _():
            take(xbuf.at[0, pl.ds(0, 28)], xs.at[0])

        @pl.when(n >= NEAR)
        def _():
            take(xbuf.at[far, group], yrm.at[n])

        @pl.when((n > 0) & (n < NEAR))
        def _():
            take(xbuf.at[far, pl.ds(n * 8, 4)], yrm.at[n])
            take(xbuf.at[far, pl.ds(n * 8 + 4, 4)], yrp.at[n])

        rows = jnp.concatenate([xbuf[k, group].reshape(128, 512) for k in range(NY)], axis=1)
        gate = dot(rows, wg[...])
        hidden = (gate * jax.nn.sigmoid(gate) * dot(rows, wu[...])).astype(bf16)
        hidden = dot(gather, hidden).astype(bf16).reshape(NY, 32, 256)
        hsend[n] = hidden
        for dy in range(1, NY):
            to = (p + dy) % NY
            remote(hsend.at[n, to], hrec.at[n, p], s_sem.at[8], hs.at[n], {"tp": to}).start()
        hrec[n, p] = hsend[n, p]

    def stage_down(n):
        take(hrec.at[n, pl.ds(0, NY - 1)], hs.at[n])
        rows = jnp.concatenate([hrec[n, k] for k in range(NY)], axis=1)
        outs = [
            dot(rows, wd[:, :, 512 * k : 512 * (k + 1)].reshape(1024, 512)).astype(bf16)
            for k in range(4)
        ]
        outs = dot(spread, jnp.concatenate(outs, axis=0)).astype(bf16).reshape(8, 16, 512)
        rsend[pl.ds(n * 8, 8)] = outs
        dz = ring_step(n)
        for j in range(8):
            device = {
                "sp_0": (z + NZ - dz) % NZ,
                "sp_1": (x + NX - j // 2) % NX,
                "sp_2": (c + j % 2) % NC,
            }

            def send(j=j, device=device):
                remote(
                    rsend.at[n * 8 + j], rbuf.at[n * 8 + j], s_sem.at[9], rs.at[n], device
                ).start()

            if j:
                send()
            else:
                pl.when(n > 0)(send)

                @pl.when(n == 0)
                def _():
                    rbuf[0] = outs[0]


    stage_forward(1)
    stage_hidden(0)
    stage_relay(1)
    stage_forward(2)
    stage_hidden(1)

    @pl.loop(3, NZ + 2)
    def _(i):
        @pl.when(i < NZ)
        def _():
            stage_forward(i)

        @pl.when(i < NZ + 1)
        def _():
            stage_relay(i - 1)

        @pl.when((i >= 4) & (i <= NEAR + 1))
        def _():
            stage_hidden(i - 2)

        @pl.when((i >= NEAR + 1) & (i < NZ + 1))
        def _():
            stage_hidden(i - 1)

        @pl.when(i == 3)
        def _():
            for n in range(4):
                take(wd.at[down, pl.ds(32 * (n + 4), 32)], wm.at[n + 4])
                take(wd.at[up, pl.ds(32 * n, 32)], wp.at[n])
            for n in range(8):
                take(wd.at[far, pl.ds(32 * n, 32)], wr.at[n])
            stage_down(0)
            stage_down(1)

        @pl.when((i >= 5) & (i <= NEAR + 2))
        def _():
            stage_down(i - 3)

        @pl.when(i >= NEAR + 2)
        def _():
            stage_down(i - 2)

    picks[...] = jnp.zeros_like(picks)
    own_rows = pl.ds(pl.multiple_of(p * GROUP, GROUP), GROUP)
    base = jnp.concatenate([dcol[0, own_rows, :], dcol[1, own_rows, :]], axis=0)
    base = base - (CAP * p).astype(f32)

    def combine(n, _):
        @pl.when(n == 0)
        def _():
            take(rbuf.at[pl.ds(1, 7)], rs.at[n])

        @pl.when(n > 0)
        def _():
            take(rbuf.at[pl.ds(n * 8, 8)], rs.at[n])

        rows = rbuf[pl.ds(n * 8, 8)].reshape(128, 512)
        for k in range(4):
            pick = jnp.where((i1 + (n * 128 - 4 * k)).astype(f32) == base, 1.0, 0.0).astype(bf16)
            picks[k] = picks[k] + dot(pick, rows)
        return 0

    lax.fori_loop(0, NZ, combine, 0)
    own = mixed[own_rows, :]
    weight = as_column(jnp.concatenate([wsel_ref[0:1, :], wsel_ref[1:2, :]], axis=1), 128)
    for k in range(4):
        cols = slice(512 * k, 512 * (k + 1))
        weighted = weight[:, 0:1] * picks[k]
        routed = weighted[0:64, :] + weighted[64:128, :]
        out_ref[:, cols] = (own[:, cols].astype(f32) + routed).astype(bf16)

    take(wd.at[pl.ds(0, 3)], s_sem.at[1])
    take(cr.at[pl.ds(0, 7)], s_sem.at[2])
    take(crd.at[pl.ds(0, 7)], s_sem.at[10])
    take(zr.at[pl.ds(0, 7)], s_sem.at[3])
    take(zrd.at[pl.ds(0, 7)], s_sem.at[11])
    take(inc.at[pl.ds(0, 7)], s_sem.at[4])
    take(gall.at[pl.ds(0, 3)], s_sem.at[5])
    take(xbuf.at[0, pl.ds(0, 28)], s_sem.at[0])
    take(xbuf.at[0, pl.ds(0, 8 * (NZ - NEAR))], s_sem.at[0])
    take(sbuf.at[pl.ds(0, 56)], s_sem.at[6])
    for k in range(2):
        take(xbuf.at[k, pl.ds(0, 8 * (NZ - 1))], s_sem.at[7])
    take(xbuf.at[2, pl.ds(0, 8 * (NEAR - 1))], s_sem.at[7])
    take(hrec.at[pl.ds(0, 6)], s_sem.at[8])
    take(rbuf.at[pl.ds(0, 63)], s_sem.at[9])


def per_device(
    stream, query, forget_gate_logits, value_input_rows, output_gate_logits, forget_floor_margin,
    additional_fading_speed, head_norm_gain, output_head_weight, feedforward_norm_gain,
    selected_expert_index, selected_expert_weight, expert_gate_weight, expert_up_weight,
    expert_down_weight,
):
    vmem = pl.BlockSpec(memory_space=pltpu.VMEM)
    hbm = pl.BlockSpec(memory_space=pl.ANY)
    dma = pltpu.SemaphoreType.DMA
    V = pltpu.VMEM
    return pl.pallas_call(
        kernel,
        name="layer",
        out_shape=jax.ShapeDtypeStruct((GROUP, 2048), bf16),
        in_specs=[vmem] * 6 + [hbm] * 9,
        out_specs=vmem,
        scratch_shapes=[
            V((ROWS, 256), bf16), V((ROWS, 256), bf16), V((ROWS, 256), bf16), V((ROWS, 256), bf16),
            V((ROWS, 2048), bf16), V((4, 256, 2048), bf16), V((2048, 256), bf16),
            V((2048, 256), bf16), V((4, 256, 2048), bf16),
            V((2, ROWS, 128), f32), V((ROWS, 256), f32), V((8, 32, 128), f32), V((8, 1, 128), f32),
            V((8, 32, 128), f32), V((8, 1, 128), f32), V((8, 32, 128), f32), V((8, 1, 128), f32),
            V((32, 128), f32), V((1, 128), f32), V((8, 32, 128), f32), V((8, 1, 128), f32),
            V((8, 32, 128), f32), V((8, 32, 128), f32), V((2, ROWS), f32), V((2, ROWS, 128), f32),
            V((4, ROWS, 256), bf16), V((ROWS, 2048), f32), V((ROWS, 2048), bf16),
            V((4, ROWS, 512), bf16), V((64, 16, 512), bf16), V((4, 64, 16, 512), bf16),
            V((8, 4, 32, 256), bf16), V((8, 4, 32, 256), bf16), V((64, 16, 512), bf16),
            V((64, 16, 512), bf16), V((4, 128, 512), f32), V((8, 8, 16, 512), bf16),
            dma((9,)), dma((12,)), dma((5,)), dma((2,)), dma((2,)), dma((2,)), dma((8,)), dma((8,)),
            dma((8,)), dma((8,)), dma((8,)), dma((8,)), dma((8,)), dma((8,)), dma((8,)), dma((8,)),
        ],
        compiler_params=pltpu.CompilerParams(
            collective_id=0, has_side_effects=True, vmem_limit_bytes=60 * 1024 * 1024
        ),
    )(
        selected_expert_index.T, selected_expert_weight.T, forget_floor_margin,
        additional_fading_speed.T, head_norm_gain.reshape(1, 128),
        feedforward_norm_gain.reshape(1, 2048), query, forget_gate_logits, value_input_rows,
        output_gate_logits, stream, output_head_weight.reshape(4, 256, 2048), expert_gate_weight[0],
        expert_up_weight[0], expert_down_weight[0],
    )


def solution(mesh):
    finer = Mesh(mesh.devices.reshape(NZ, NX, NC, mesh.shape["tp"]), SP_TP)
    in_specs = (
        P(SP, None), P(SP, "tp"), P(SP, "tp"), P(SP, "tp"), P(SP, "tp"), P("tp", None),
        P(SP, "tp"), P(), P(), P(), P(SP, None), P(SP_TP, None), P(SP, None, "tp"),
        P(SP, None, "tp"), P(SP, "tp", None),
    )
    return jax.shard_map(
        per_device, mesh=finer, in_specs=in_specs, out_specs=P(SP_TP, None), check_vma=False
    )
```
